256 devices in a mesh: sp: 64 (over z, x, core), tp: 4 (over y).
Axes of the slice: x: 4, y: 4, z: 8, core: 2. Of those that a mesh axis runs over, the one named last changes fastest.
Arguments:
- tokens: bfloat16 [16384, 2048], P(('sp', 'tp')), may hold values from -6 to 6
- query_weight: bfloat16 [2048, 2048], P('sp', 'tp'), may hold values from -0.125 to 0.125
- key_weight: bfloat16 [2048, 512], P('sp', 'tp'), may hold values from -0.125 to 0.125
- value_weight: bfloat16 [2048, 512], P('sp', 'tp'), may hold values from -0.125 to 0.125
- out_weight: bfloat16 [2048, 2048], P('tp', 'sp'), may hold values from -0.125 to 0.125
- query_gain: float32 [128], replicated, may hold values from 0.1 to 1.9
- key_gain: float32 [128], replicated, may hold values from 0.1 to 1.9
Outputs:
- mixed: bfloat16 [16384, 2048], P(('sp', 'tp'))
The draws below stay inside these ranges and needn't reach their ends.
All inputs are finite; a program needn't handle non-finite values.
Results may differ from the reference program's by a relative error of at most 0.02.
Values may be sent and summed in bfloat16 or wider, within the bound.
No kernel may reach another device: no remote copies, remote signals or barrier semaphores. Data moves between devices by JAX's collectives and lax.ppermute only.
A program may use at most 64 MiB of HBM per device.

```python
import math
import jax
import jax.numpy as jnp
from jax import lax

D = 2048
HEAD_DIM = 128
Q_HEADS = 16
KV_HEADS = 4
GROUP = 4
GRID_W = 64
TOKENS = 16384


def block_scale(rng, shape, cuts, least, high):
    level, own = 1.0, jax.random.fold_in(rng, 6)
    for position, blocks in cuts:
        heights = jnp.exp(jax.random.uniform(jax.random.fold_in(own, position), (blocks,), jnp.float32, least / len(cuts), high / len(cuts)))
        level = level * jnp.repeat(heights, shape[position] // blocks).reshape([-1 if axis == position else 1 for axis in range(len(shape))])
    return level


def noise(rng, extent, width, bound, shards=(), held_as=jnp.bfloat16):
    result = jax.random.normal(rng, extent, jnp.float32) * width
    if len(shards) > 0:
        result = block_scale(rng, extent, shards, -0.22, 0.18) * result
    return jnp.clip(result, min=-bound, max=bound).astype(held_as)


def setup_inputs(seed: int = 0) -> dict:
    key_list = jax.random.split(jax.random.key(seed), 8)
    tokens = noise(key_list[0], (TOKENS, D), 1.0, 6.0, ((0, 256),))
    query_weight = noise(key_list[1], (D, Q_HEADS * HEAD_DIM), D ** -0.5, 0.125, ((0, 64), (1, 4)))
    key_weight = noise(key_list[2], (D, KV_HEADS * HEAD_DIM), D ** -0.5, 0.125, ((0, 64), (1, 4)))
    value_weight = noise(key_list[3], (D, KV_HEADS * HEAD_DIM), D ** -0.5, 0.125, ((0, 64), (1, 4)))
    out_weight = noise(key_list[4], (Q_HEADS * HEAD_DIM, D), (Q_HEADS * HEAD_DIM) ** -0.5, 0.125, ((0, 4), (1, 64)))
    query_gain = jnp.clip(1.0 + 0.18 * jax.random.normal(key_list[5], (HEAD_DIM,), jnp.float32), 0.1, 1.9)
    key_gain = jnp.clip(1.0 + 0.18 * jax.random.normal(key_list[6], (HEAD_DIM,), jnp.float32), 0.1, 1.9)
    return dict(tokens=tokens, query_weight=query_weight, key_weight=key_weight, value_weight=value_weight, out_weight=out_weight, query_gain=query_gain, key_gain=key_gain)


eps = 1e-06
rope_base = 10000.0

def normalize(raw, gain):
    wide = raw.astype(jnp.float32)
    return wide * lax.rsqrt(lax.optimization_barrier(jnp.mean(wide * wide, axis=-1, keepdims=True)) + eps) * gain

def rotate(values_in, positions):
    pair_count = values_in.shape[-1] // 4
    inverse_rate = rope_base ** (-jnp.arange(0, 2 * pair_count, 2, dtype=jnp.float32) / (2 * pair_count))
    grid_row = (positions // GRID_W).astype(jnp.float32)
    grid_column = (positions % GRID_W).astype(jnp.float32)
    angles = jnp.stack([grid_row[:, None] * inverse_rate, grid_column[:, None] * inverse_rate], axis=1)
    cosine = jnp.cos(angles)[:, None]
    sine = jnp.sin(angles)[:, None]
    shaped = values_in.reshape(values_in.shape[:-1] + (2, 2, pair_count))
    leading = shaped[..., 0, :]
    trailing = shaped[..., 1, :]
    turned = jnp.stack([leading * cosine - trailing * sine, trailing * cosine + leading * sine], axis=-2)
    return turned.reshape(values_in.shape)

def reference(tokens, query_weight, key_weight, value_weight, out_weight, query_gain, key_gain):
    rows = tokens.shape[0]

    def project(weight, heads):
        return jnp.dot(tokens, weight, preferred_element_type=jnp.float32).astype(jnp.bfloat16).reshape(rows, heads, HEAD_DIM)
    positions = jnp.arange(rows, dtype=jnp.int32)
    queries = rotate(normalize(project(query_weight, Q_HEADS), query_gain), positions).astype(jnp.bfloat16)
    keys = rotate(normalize(project(key_weight, KV_HEADS), key_gain), positions).astype(jnp.bfloat16)
    values = project(value_weight, KV_HEADS)
    block = math.gcd(rows, 128)
    grouped = queries.reshape(rows // block, block, KV_HEADS, GROUP, HEAD_DIM)
    scale = HEAD_DIM ** (-0.5)

    def one_block(query_block):
        scores = jnp.einsum('qkgd,skd->kgqs', query_block, keys, preferred_element_type=jnp.float32) * scale
        highest = lax.optimization_barrier(jnp.max(scores, axis=-1, keepdims=True))
        exponentials = jnp.exp(scores - highest)
        total = lax.optimization_barrier(jnp.sum(exponentials, axis=-1))
        weights = exponentials.astype(jnp.bfloat16)
        summed = jnp.einsum('kgqs,skd->kgqd', weights, values, preferred_element_type=jnp.float32)
        return jnp.transpose(summed / total[..., None], (2, 0, 1, 3))
    attended = lax.map(one_block, grouped).reshape(rows, Q_HEADS * HEAD_DIM).astype(jnp.bfloat16)
    projected = jnp.dot(attended, out_weight, preferred_element_type=jnp.float32)
    scaled = projected * lax.rsqrt(lax.optimization_barrier(jnp.mean(projected * projected, axis=-1, keepdims=True)) + eps)
    return scaled.astype(jnp.bfloat16)
```

```python
import functools
import math

import jax
import jax.numpy as jnp
from jax import lax
from jax.experimental import pallas as pl
from jax.experimental.pallas import tpu as pltpu
from jax.sharding import Mesh
from jax.sharding import PartitionSpec as P

HEAD_DIM = 128
GROUP = 4
GRID_W = 64
Z, X, C, Y = "sp_0", "sp_1", "sp_2", "tp"
SP = (Z, X, C)
SP_TP = (Z, X, C, Y)

eps = 1e-06
rope_base = 10000.0

F32 = jnp.float32
BF16 = jnp.bfloat16


def everyone(piece, axes):
    n = lax.axis_size(axes)
    return lax.all_to_all(jnp.broadcast_to(piece[None], (n,) + piece.shape), axes, 0, 0)


def other_core(piece):
    return lax.ppermute(piece, C, [(0, 1), (1, 0)])


def both_cores(own):
    other = other_core(own)
    first = lax.axis_index(C) == 0
    return jnp.stack([jnp.where(first, own, other), jnp.where(first, other, own)], axis=1)


def ring_step(block):
    n = lax.axis_size(Z)
    pairs = [(i * 2, (i + 1) % n * 2) for i in range(n)] + [(i * 2 + 1, (i - 1) % n * 2 + 1) for i in range(n)]
    return lax.ppermute(block, (Z, C), pairs)


def tables(positions):
    lane = jnp.arange(HEAD_DIM)
    f = lane % 32
    inverse_rate = rope_base ** (-(2 * f).astype(F32) / 64)
    row = (positions // GRID_W).astype(F32)
    column = (positions % GRID_W).astype(F32)
    place = jnp.where(lane[None] < 64, row[:, None], column[:, None])
    angle = place * inverse_rate[None]
    return jnp.cos(angle), jnp.sin(angle) * jnp.where((lane // 32) % 2 == 0, -1.0, 1.0)


def normalize_rotate(raw, gain, cosine, sine, scale):
    rows, width = raw.shape
    out = []
    for h in range(width // HEAD_DIM):
        wide = raw[:, h * HEAD_DIM : (h + 1) * HEAD_DIM].astype(F32)
        n = wide * lax.rsqrt(jnp.mean(wide * wide, axis=-1, keepdims=True) + eps) * gain
        swapped = jnp.concatenate([n[:, 32:64], n[:, :32], n[:, 96:], n[:, 64:96]], axis=1)
        out.append(((n * cosine + swapped * sine) * scale).astype(BF16))
    return out


def attend_kernel(*refs, sub, first):
    if first:
        q_ref, kv_ref, m_ref, a_ref, v_ref = refs
    else:
        q_ref, kv_ref, mi_ref, ai_ref, m_ref, a_ref, v_ref = refs
    count = kv_ref.shape[0]
    rows = q_ref.shape[0]

    @pl.when(pl.program_id(0) == 0)
    def _():
        v_ref[:, :HEAD_DIM] = kv_ref[:, HEAD_DIM:]
        v_ref[:, HEAD_DIM:] = jnp.ones((count, HEAD_DIM), BF16)

    def scores(r):
        return lax.dot_general(
            q_ref[r : r + sub], kv_ref[:, :HEAD_DIM], (((1,), (1,)), ((), ())), preferred_element_type=F32
        )

    following = scores(0)
    for r in range(0, rows, sub):
        s = following
        if r + sub < rows:
            following = scores(r + sub)
        best = jnp.max(s, axis=1, keepdims=True)
        if not first:
            old = mi_ref[r : r + sub, :1]
            best = jnp.maximum(best, old)
        weights = jnp.exp2(s - best).astype(BF16)
        acc = jnp.dot(weights, v_ref[...], preferred_element_type=F32)
        if not first:
            acc = acc + ai_ref[r : r + sub] * jnp.exp2(old - best)
        m_ref[r : r + sub] = jnp.broadcast_to(best, (sub, HEAD_DIM))
        a_ref[r : r + sub] = acc


def attend(q, kv, carry):
    m_rows, count = q.shape[0], kv.shape[0]
    rows, sub = 1024, 128 if count > 1024 else 256
    first = carry is None
    row_spec = pl.BlockSpec((rows, HEAD_DIM), lambda i: (i, 0))
    acc_spec = pl.BlockSpec((rows, 2 * HEAD_DIM), lambda i: (i, 0))
    return pl.pallas_call(
        functools.partial(attend_kernel, sub=sub, first=first),
        grid=(m_rows // rows,),
        in_specs=[row_spec, pl.BlockSpec((count, 2 * HEAD_DIM), lambda i: (0, 0))]
        + ([] if first else [row_spec, acc_spec]),
        out_specs=[row_spec, acc_spec],
        out_shape=[
            jax.ShapeDtypeStruct((m_rows, HEAD_DIM), F32),
            jax.ShapeDtypeStruct((m_rows, 2 * HEAD_DIM), F32),
        ],
        scratch_shapes=[pltpu.VMEM((count, 2 * HEAD_DIM), BF16)],
        input_output_aliases={} if first else {2: 0, 3: 1},
        compiler_params=pltpu.CompilerParams(dimension_semantics=("arbitrary",), vmem_limit_bytes=40 * 2**20),
        cost_estimate=pl.CostEstimate(
            flops=8 * m_rows * count * HEAD_DIM, bytes_accessed=8 * 2**20, transcendentals=m_rows * count
        ),
        name="attend",
    )(q, kv, *([] if first else carry))


def local(tokens, query_weight, key_weight, value_weight, out_weight, query_gain, key_gain):
    kv_shard = jnp.concatenate([key_weight, value_weight], axis=1)
    chips = (Z, X)
    kv_weight = both_cores(everyone(kv_shard, chips)).reshape(-1, 2 * HEAD_DIM)
    rows_in = everyone(tokens, Y).reshape(-1, tokens.shape[1])
    rows = rows_in.shape[0]
    q_weight = both_cores(everyone(query_weight, chips)).reshape(-1, query_weight.shape[1])
    w_out = both_cores(everyone(out_weight.T, chips)).reshape(-1, out_weight.shape[0])

    positions = lax.axis_index(SP) * rows + jnp.arange(rows, dtype=jnp.int32)
    cosine, sine = tables(positions)

    kv_raw = jnp.dot(rows_in, kv_weight, preferred_element_type=F32).astype(BF16)
    key = normalize_rotate(kv_raw[:, :HEAD_DIM], key_gain, cosine, sine, 1.0)[0]
    kv_own = jnp.concatenate([key, kv_raw[:, HEAD_DIM:]], axis=1)
    plane = everyone(kv_own, X).reshape(-1, 2 * HEAD_DIM)
    block = jnp.concatenate([plane, other_core(plane)], axis=0)

    q_raw = jnp.dot(rows_in, q_weight, preferred_element_type=F32).astype(BF16)
    scale = HEAD_DIM ** (-0.5) * math.log2(math.e)
    q_own = jnp.concatenate(normalize_rotate(q_raw, query_gain, cosine, sine, scale), axis=0)
    q_all = jnp.concatenate([q_own, other_core(q_own)], axis=0)

    carry = None
    held = plane
    turns = lax.axis_size(Z) // 2
    for step in range(turns + 1):
        if step < turns:
            coming = ring_step(block if step < turns - 1 else block[: block.shape[0] // 2])
        carry = attend(q_all, held, carry)
        block = held = coming
    best, acc = carry
    half = q_own.shape[0]
    sent = jnp.concatenate([best[half:], acc[half:]], axis=1)
    got = other_core(sent)
    best_a, acc_a = best[:half], acc[:half]
    best_b, acc_b = got[:, :HEAD_DIM], got[:, HEAD_DIM:]
    top = jnp.maximum(best_a, best_b)
    wa, wb = jnp.exp2(best_a - top), jnp.exp2(best_b - top)
    numerator = acc_a[:, :HEAD_DIM] * wa + acc_b[:, :HEAD_DIM] * wb
    total = acc_a[:, HEAD_DIM:] * wa + acc_b[:, HEAD_DIM:] * wb
    attended = (numerator / total).astype(BF16)
    attended = jnp.concatenate([attended[h * rows : (h + 1) * rows] for h in range(GROUP)], axis=1)

    partial = lax.dot_general(attended, w_out, (((1,), (1,)), ((), ())), preferred_element_type=F32)
    pieces = partial.astype(BF16).reshape(lax.axis_size(Y), -1, partial.shape[1])
    summed = jnp.sum(lax.all_to_all(pieces, Y, 0, 0).astype(F32), axis=0)
    mixed = summed * lax.rsqrt(jnp.mean(summed * summed, axis=-1, keepdims=True) + eps)
    return mixed.astype(BF16)


def solution(mesh):
    split = Mesh(mesh.devices.reshape(8, 4, 2, mesh.shape["tp"]), SP_TP)
    return jax.shard_map(
        local,
        mesh=split,
        in_specs=(P(SP_TP, None), P(SP, Y), P(SP, Y), P(SP, Y), P(Y, SP), P(), P()),
        out_specs=P(SP_TP, None),
        check_vma=False,
    )
```

```python
import functools
import math

import jax
import jax.numpy as jnp
from jax import lax
from jax.experimental import pallas as pl
from jax.experimental.pallas import tpu as pltpu
from jax.sharding import Mesh
from jax.sharding import PartitionSpec as P


HEAD_DIM = 128
GROUP = 4
GRID_W = 64
Z, X, C, Y = "sp_0", "sp_1", "sp_2", "tp"
SP = (Z, X, C)
SP_TP = (Z, X, C, Y)
NZ, NX, NC, NY = 8, 4, 2, 4

eps = 1e-06
rope_base = 10000.0

F32 = jnp.float32
BF16 = jnp.bfloat16
WHOLE = pl.BlockSpec(memory_space=pltpu.VMEM)
SCALARS = pl.BlockSpec(memory_space=pltpu.SMEM)


def other_core(piece):
    return lax.ppermute(piece, C, [(0, 1), (1, 0)])


def turn(piece, axis, count):
    pairs = []
    for i in range(count):
        pairs += [(i * 2, (i + 1) % count * 2), (i * 2 + 1, (i - 1) % count * 2 + 1)]
    return lax.ppermute(piece, (axis, C), pairs)


def shift(piece, axis, count, by):
    return lax.ppermute(piece, axis, [(i, (i + by) % count) for i in range(count)])


def leap(piece, by):
    pairs = []
    for i in range(NZ):
        pairs += [(i * 2, (i + by) % NZ * 2), (i * 2 + 1, (i - by) % NZ * 2 + 1)]
    return lax.ppermute(piece, (Z, C), pairs)


def everyone(piece, axes):
    n = lax.axis_size(axes)
    return lax.all_to_all(jnp.broadcast_to(piece[None], (n,) + piece.shape), axes, 0, 0)


def after(value, *events):
    return lax.optimization_barrier((value, *events))[0]


def call(kernel, outs, *args, scratch=(), flops=0):
    return pl.pallas_call(
        kernel,
        in_specs=[SCALARS] + [WHOLE] * (len(args) - 1),
        out_specs=[WHOLE] * len(outs),
        out_shape=[jax.ShapeDtypeStruct(s, d) for s, d in outs],
        scratch_shapes=list(scratch),
        compiler_params=pltpu.CompilerParams(vmem_limit_bytes=40 * 2**20),
        cost_estimate=pl.CostEstimate(flops=flops, bytes_accessed=4 * 2**20, transcendentals=0),
    )(*args)


def at(index, size):
    return pl.ds(pl.multiple_of(index * size, size), size)


def column_kernel(i_ref, own_ref, other_ref, mine_ref, got_ref, out_ref, half_ref):
    z, c = i_ref[0], i_ref[2]
    away = 1 - 2 * c

    def put(rows, plane, half):
        out_ref[at(half * NZ + (plane + 2 * NZ) % NZ, 32), :] = rows

    put(own_ref[...], z, c)
    put(other_ref[...], z, 1 - c)
    for s in range(1, 4):
        for j in range(2):
            half = jnp.where(c == 0, j, 1 - j)
            place = slice(s * 64 - 64 + j * 32, s * 64 - 32 + j * 32)
            put(mine_ref[place], z - away * s, half)
            put(got_ref[place], z + away * s, 1 - half)
    put(mine_ref[192:], z + 4, c)
    put(got_ref[192:], z + 4, 1 - c)
    half_ref[...] = out_ref[at(c, 256), :]


def fill_rows(i_ref, w_ref, column, near, near_got, far, far_got):
    x, c = i_ref[1], i_ref[2]
    minus = (x + jnp.where(c == 0, 3, 1)) % NX
    plus = (x + jnp.where(c == 0, 1, 3)) % NX
    opposite = (x + 2) % NX

    def plane(z, nothing):
        for k in range(2):
            place = pl.ds(pl.multiple_of(z * 32, 32) + k * 256, 32)
            for ref, where in ((column, x), (near, minus), (near_got, plus)):
                w_ref[at((z * NX + where) * 2 + k, 32), :] = ref[place, :]
        w_ref[at((z * NX + opposite) * 2 + c, 32), :] = far[at(z, 32), :]
        w_ref[at((z * NX + opposite) * 2 + 1 - c, 32), :] = far_got[at(z, 32), :]
        return nothing

    lax.fori_loop(0, NZ, plane, 0)


def rotated(raw, gain, cosine, sine, scale):
    wide = raw.astype(F32)
    n = wide * lax.rsqrt(jnp.mean(wide * wide, axis=-1, keepdims=True) + eps) * gain
    lane = lax.broadcasted_iota(jnp.int32, n.shape, 1)
    swapped = jnp.where(lane // 32 % 2 == 0, pltpu.roll(n, 96, 1), pltpu.roll(n, 32, 1))
    return ((n * cosine + swapped * sine) * scale).astype(BF16)


def kv_kernel(i_ref, t0, t1, t2, t3, own, got, gain, cosine, sine, kv_ref, t_ref, w_ref):
    c, y = i_ref[2], i_ref[3]
    for by, ref in enumerate((t0, t1, t2, t3)):
        t_ref[at((y + by) % NY, 64), :] = ref[...]

    def chip(i, nothing):
        for k in range(4):
            w_ref[at((i * 4 + k) * 2 + c, 32), :] = own[i * 4 + k]
            w_ref[at((i * 4 + k) * 2 + 1 - c, 32), :] = got[i * 4 + k]
        return nothing

    lax.fori_loop(0, NZ * NX // 4, chip, 0)
    raw = jnp.dot(t_ref[...], w_ref[...], preferred_element_type=F32).astype(BF16)
    kv_ref[:, :HEAD_DIM] = rotated(raw[:, :HEAD_DIM], gain[...], cosine[...], sine[...], 1.0)
    kv_ref[:, HEAD_DIM:] = raw[:, HEAD_DIM:]


def q_kernel(i_ref, t_ref, column, near, near_got, far, far_got, gain, cosine, sine, q_ref, w_ref):
    fill_rows(i_ref, w_ref, column, near, near_got, far, far_got)
    raw = jnp.dot(t_ref[...], w_ref[...], preferred_element_type=F32).astype(BF16)
    rows = raw.shape[0]
    scale = HEAD_DIM ** (-0.5) * math.log2(math.e)
    for h in range(GROUP):
        head = raw[:, h * HEAD_DIM : (h + 1) * HEAD_DIM]
        q_ref[h * rows : (h + 1) * rows, :] = rotated(head, gain[...], cosine[...], sine[...], scale)


def attend_kernel(*refs, sub, chunk, first, last, offset):
    if first:
        q_ref, kv_ref, m_ref, a_ref, v_ref = refs
    elif last:
        q_ref, kv_ref, mi_ref, ai_ref, a_ref, v_ref = refs
    else:
        q_ref, kv_ref, mi_ref, ai_ref, m_ref, a_ref, v_ref = refs
    v_ref[:, :HEAD_DIM] = kv_ref[:, HEAD_DIM:]
    v_ref[:, HEAD_DIM:] = jnp.ones((kv_ref.shape[0], HEAD_DIM), BF16)
    lane = lax.broadcasted_iota(jnp.int32, (sub, HEAD_DIM), 1)

    def part(t, nothing):
        def rows(r, base=offset):
            return pl.ds(pl.multiple_of(t * chunk + r, sub) + base, sub)

        def scores(r):
            return lax.dot_general(
                q_ref[rows(r)], kv_ref[:, :HEAD_DIM], (((1,), (1,)), ((), ())), preferred_element_type=F32
            )

        following = scores(0)
        for r in range(0, chunk, sub):
            s = following
            if r + sub < chunk:
                following = scores(r + sub)
            best = jnp.max(s, axis=1, keepdims=True)
            if not first:
                old = mi_ref[rows(r), :1]
                best = jnp.maximum(best, old)
            weights = jnp.exp2(s - best).astype(BF16)
            acc = jnp.dot(weights, v_ref[...], preferred_element_type=F32)
            if not first:
                acc = acc + ai_ref[rows(r)] * jnp.exp2(old - best)
            if last:
                a_ref[rows(r, 0), :HEAD_DIM] = acc[:, :HEAD_DIM]
                a_ref[rows(r, 0), HEAD_DIM:] = jnp.where(lane < 64, acc[:, HEAD_DIM:], best)
            else:
                m_ref[rows(r)] = jnp.broadcast_to(best, (sub, HEAD_DIM))
                a_ref[rows(r)] = acc
        return nothing

    steps = a_ref.shape[0] // chunk
    if steps == 1:
        part(0, 0)
    else:
        lax.fori_loop(0, steps, part, 0)


def attend(q, kv, carry, last=None):
    first, count = carry is None, kv.shape[0]
    rows = q.shape[0] // (1 if last is None else 2)
    shapes = [jax.ShapeDtypeStruct((rows, n), F32) for n in ((HEAD_DIM, 2 * HEAD_DIM) if last is None else (2 * HEAD_DIM,))]
    out = pl.pallas_call(
        functools.partial(
            attend_kernel, sub=128, chunk=1024, first=first, last=last is not None, offset=(last or 0) * rows
        ),
        in_specs=[WHOLE] * (2 if first else 4),
        out_specs=[WHOLE] * len(shapes),
        out_shape=shapes,
        scratch_shapes=[pltpu.VMEM((count, 2 * HEAD_DIM), BF16)],
        input_output_aliases={} if first or last is not None else {2: 0, 3: 1},
        compiler_params=pltpu.CompilerParams(vmem_limit_bytes=40 * 2**20),
        cost_estimate=pl.CostEstimate(
            flops=8 * rows * count * HEAD_DIM, bytes_accessed=8 * 2**20, transcendentals=rows * count
        ),
        name="attend",
    )(q, kv, *([] if first else carry))
    return out if last is None else out[0]


def project_out_kernel(i_ref, own_ref, got_ref, column, near, near_got, far, far_got, out_ref, w_ref, at_ref):
    fill_rows(i_ref, w_ref, column, near, near_got, far, far_got)
    rows = own_ref.shape[0] // GROUP
    for h in range(GROUP):
        mine, theirs = own_ref[h * rows : (h + 1) * rows], got_ref[h * rows : (h + 1) * rows]
        best_a, best_b = mine[:, 255:256], theirs[:, 255:256]
        top = jnp.maximum(best_a, best_b)
        both = mine * jnp.exp2(best_a - top) + theirs * jnp.exp2(best_b - top)
        at_ref[:, h * HEAD_DIM : (h + 1) * HEAD_DIM] = (both[:, :HEAD_DIM] / both[:, HEAD_DIM : HEAD_DIM + 1]).astype(BF16)
    out_ref[...] = lax.dot_general(
        at_ref[...], w_ref[...], (((1,), (1,)), ((), ())), preferred_element_type=F32
    ).astype(BF16)


def tables(positions):
    lane = jnp.arange(HEAD_DIM)
    f = lane % 32
    inverse_rate = rope_base ** (-(2 * f).astype(F32) / 64)
    row = (positions // GRID_W).astype(F32)
    column = (positions % GRID_W).astype(F32)
    place = jnp.where(lane[None] < 64, row[:, None], column[:, None])
    angle = place * inverse_rate[None]
    return jnp.cos(angle), jnp.sin(angle) * jnp.where((lane // 32) % 2 == 0, -1.0, 1.0)


def from_z(where, own, other):
    slab = jnp.concatenate([own, other], axis=0)
    mine = jnp.concatenate([leap(slab, 1), leap(slab, 2), leap(slab, 3), leap(own, 4)], axis=0)
    return call(column_kernel, [((512, 512), BF16), ((256, 512), BF16)], where, own, other, mine, other_core(mine))


def from_x(column, half):
    near, far = turn(column, X, NX), shift(half, X, NX, 2)
    return column, near, other_core(near), far, other_core(far)


def local(tokens, query_weight, key_weight, value_weight, out_weight, query_gain, key_gain):
    where = jnp.stack([lax.axis_index(a) for a in (Z, X, C, Y)]).astype(jnp.int32)
    rows = tokens.shape[0] * NY
    positions = lax.axis_index(SP) * rows + jnp.arange(rows, dtype=jnp.int32)
    cosine, sine = tables(positions)
    gain_q, gain_k = query_gain[None], key_gain[None]

    wo_own = out_weight.T
    q_other, wo_other = other_core(query_weight), other_core(wo_own)
    kv_weight = everyone(after(jnp.concatenate([key_weight, value_weight], axis=1), q_other), (Z, X))
    kv_weight = after(kv_weight, wo_other)
    q_column, q_half = from_z(where, query_weight, q_other)
    toks = [tokens] + [shift(tokens, Y, NY, -by) for by in (1, 2, 3)]

    kv_own, rows_in = call(
        kv_kernel, [((rows, 256), BF16), ((rows, tokens.shape[1]), BF16)],
        where, *toks, kv_weight, other_core(kv_weight), gain_k, cosine, sine,
        scratch=[pltpu.VMEM((tokens.shape[1], 256), BF16)],
    )
    kv_slab = jnp.concatenate([kv_own, other_core(kv_own)], axis=0)
    kv_near, kv_far = turn(kv_slab, X, NX), shift(kv_own, X, NX, 2)
    plane = jnp.concatenate([kv_own, kv_near, kv_far], axis=0)

    q_column, q_half = after((q_column, q_half), kv_slab)
    wo_own, wo_other = after((wo_own, wo_other), kv_own)
    wo_column, wo_half = from_z(where, wo_own, wo_other)

    (q_own,) = call(
        q_kernel, [((GROUP * rows, HEAD_DIM), BF16)],
        where, rows_in, *from_x(q_column, q_half), gain_q, cosine, sine,
        scratch=[pltpu.VMEM((tokens.shape[1], 512), BF16)],
    )
    q_all = jnp.concatenate([q_own, other_core(q_own)], axis=0)
    wo_all = from_x(*after((wo_column, wo_half), q_own))

    chain = {"a": plane, "b": other_core(plane)}
    carry, todo = None, [plane]
    for step in range(1, 5):
        for name in "ab" if step < 4 else "a":
            chain[name] = turn(chain[name], Z, NZ)
            todo.append(chain[name])
    for piece in todo[:-1]:
        carry = attend(q_all, piece, carry)
    theirs = attend(q_all, todo[-1], carry, last=1)
    got = other_core(theirs)
    own = attend(q_all, todo[-1], carry, last=0)
    (partial,) = call(
        project_out_kernel, [((rows, tokens.shape[1]), BF16)], where, own, got, *wo_all,
        scratch=[pltpu.VMEM((2048, 512), BF16), pltpu.VMEM((rows, GROUP * HEAD_DIM), BF16)],
    )
    pieces = partial.reshape(NY, -1, partial.shape[1])
    summed = jnp.sum(lax.all_to_all(pieces, Y, 0, 0).astype(F32), axis=0)
    mixed = summed * lax.rsqrt(jnp.mean(summed * summed, axis=-1, keepdims=True) + eps)
    return mixed.astype(BF16)


def solution(mesh):
    split = Mesh(mesh.devices.reshape(NZ, NX, NC, NY), SP_TP)

    return jax.shard_map(
        local,
        mesh=split,
        in_specs=(P(SP_TP, None), P(SP, Y), P(SP, Y), P(SP, Y), P(Y, SP), P(), P()),
        out_specs=P(SP_TP, None),
        check_vma=False,
    )
```

```python
import functools
import math

import jax
import jax.numpy as jnp
from jax import lax
from jax.experimental import pallas as pl
from jax.experimental.pallas import tpu as pltpu
from jax.sharding import Mesh
from jax.sharding import PartitionSpec as P


HEAD_DIM = 128
GROUP = 4
GRID_W = 64
Z, X, C, Y = "sp_0", "sp_1", "sp_2", "tp"
SP = (Z, X, C)
SP_TP = (Z, X, C, Y)
NZ, NX, NC, NY = 8, 4, 2, 4

eps = 1e-06
rope_base = 10000.0

F32 = jnp.float32
BF16 = jnp.bfloat16
WHOLE = pl.BlockSpec(memory_space=pltpu.VMEM)
SCALARS = pl.BlockSpec(memory_space=pltpu.SMEM)


def other_core(piece):
    return lax.ppermute(piece, C, [(0, 1), (1, 0)])


def turn(piece, axis, count):
    pairs = []
    for i in range(count):
        pairs += [(i * 2, (i + 1) % count * 2), (i * 2 + 1, (i - 1) % count * 2 + 1)]
    return lax.ppermute(piece, (axis, C), pairs)


def shift(piece, axis, count, by):
    return lax.ppermute(piece, axis, [(i, (i + by) % count) for i in range(count)])


def leap(piece, by):
    pairs = []
    for i in range(NZ):
        pairs += [(i * 2, (i + by) % NZ * 2), (i * 2 + 1, (i - by) % NZ * 2 + 1)]
    return lax.ppermute(piece, (Z, C), pairs)


def everyone(piece, axes):
    n = lax.axis_size(axes)
    return lax.all_to_all(jnp.broadcast_to(piece[None], (n,) + piece.shape), axes, 0, 0)


def after(value, *events):
    return lax.optimization_barrier((value, *events))[0]


def call(kernel, outs, *args, scratch=(), flops=0):
    return pl.pallas_call(
        kernel,
        in_specs=[SCALARS] + [WHOLE] * (len(args) - 1),
        out_specs=[WHOLE] * len(outs),
        out_shape=[jax.ShapeDtypeStruct(s, d) for s, d in outs],
        scratch_shapes=list(scratch),
        compiler_params=pltpu.CompilerParams(vmem_limit_bytes=40 * 2**20),
        cost_estimate=pl.CostEstimate(flops=flops, bytes_accessed=4 * 2**20, transcendentals=0),
    )(*args)


def at(index, size):
    return pl.ds(pl.multiple_of(index * size, size), size)


def column_kernel(i_ref, own_ref, other_ref, mine_ref, got_ref, q_ref, q_half_ref, o_ref, o_half_ref):
    z, c = i_ref[0], i_ref[2]
    away = 1 - 2 * c
    width = q_ref.shape[1]

    def put(ref, start, plane, half):
        place = at(half * NZ + (plane + 2 * NZ) % NZ, 32)
        q_ref[place, :] = ref[start : start + 32, :width]
        o_ref[place, :] = ref[start : start + 32, width:]

    put(own_ref, 0, z, c)
    put(other_ref, 0, z, 1 - c)
    for s in range(1, 4):
        for j in range(2):
            half = jnp.where(c == 0, j, 1 - j)
            start = s * 64 - 64 + j * 32
            put(mine_ref, start, z - away * s, half)
            put(got_ref, start, z + away * s, 1 - half)
    put(mine_ref, 192, z + 4, c)
    put(got_ref, 192, z + 4, 1 - c)
    q_half_ref[...] = q_ref[at(c, 256), :]
    o_half_ref[...] = o_ref[at(c, 256), :]


def fill_rows(i_ref, w_ref, column, rest, got):
    x, c = i_ref[1], i_ref[2]
    minus = (x + jnp.where(c == 0, 3, 1)) % NX
    plus = (x + jnp.where(c == 0, 1, 3)) % NX
    opposite = (x + 2) % NX

    def plane(z, nothing):
        row = pl.multiple_of(z * 32, 32)
        for k in range(2):
            place = pl.ds(row + k * 256, 32)
            for ref, where in ((column, x), (rest, minus), (got, plus)):
                w_ref[at((z * NX + where) * 2 + k, 32), :] = ref[place, :]
        w_ref[at((z * NX + opposite) * 2 + c, 32), :] = rest[pl.ds(row + 512, 32), :]
        w_ref[at((z * NX + opposite) * 2 + 1 - c, 32), :] = got[pl.ds(row + 512, 32), :]
        return nothing

    lax.fori_loop(0, NZ, plane, 0)


def rotated(raw, gain, cosine, sine, scale):
    wide = raw.astype(F32)
    n = wide * lax.rsqrt(jnp.mean(wide * wide, axis=-1, keepdims=True) + eps) * gain
    lane = lax.broadcasted_iota(jnp.int32, n.shape, 1)
    swapped = jnp.where(lane // 32 % 2 == 0, pltpu.roll(n, 96, 1), pltpu.roll(n, 32, 1))
    return ((n * cosine + swapped * sine) * scale).astype(BF16)


def kv_kernel(i_ref, t0, t1, t2, t3, own, got, gain, cosine, sine, kv_ref, t_ref, w_ref):
    c, y = i_ref[2], i_ref[3]
    for by, ref in enumerate((t0, t1, t2, t3)):
        t_ref[at((y + by) % NY, 64), :] = ref[...]

    def chip(i, nothing):
        for k in range(4):
            w_ref[at((i * 4 + k) * 2 + c, 32), :] = own[i * 4 + k]
            w_ref[at((i * 4 + k) * 2 + 1 - c, 32), :] = got[i * 4 + k]
        return nothing

    lax.fori_loop(0, NZ * NX // 4, chip, 0)
    raw = jnp.dot(t_ref[...], w_ref[...], preferred_element_type=F32).astype(BF16)
    kv_ref[:, :HEAD_DIM] = rotated(raw[:, :HEAD_DIM], gain[...], cosine[...], sine[...], 1.0)
    kv_ref[:, HEAD_DIM:] = raw[:, HEAD_DIM:]


def q_kernel(i_ref, t_ref, column, rest, got, gain, cosine, sine, q_ref, w_ref):
    fill_rows(i_ref, w_ref, column, rest, got)
    raw = jnp.dot(t_ref[...], w_ref[...], preferred_element_type=F32).astype(BF16)
    rows = raw.shape[0]
    scale = HEAD_DIM ** (-0.5) * math.log2(math.e)
    for h in range(GROUP):
        head = raw[:, h * HEAD_DIM : (h + 1) * HEAD_DIM]
        q_ref[h * rows : (h + 1) * rows, :] = rotated(head, gain[...], cosine[...], sine[...], scale)


def attend_kernel(*refs, pieces, first, last, offset):
    q_ref, *kv_refs = refs[: 1 + pieces]
    ins = refs[1 + pieces : 1 + pieces + (0 if first else 2)]
    *outs, k_ref, v_ref = refs[1 + pieces + len(ins) :]
    out_ref, m_ref, a_ref = outs if last else (None, *outs)
    if first:
        m_ref[...] = jnp.full(m_ref.shape, -1e30, F32)
        a_ref[...] = jnp.zeros(a_ref.shape, F32)
    else:
        kept = slice(offset, offset + m_ref.shape[0])
        m_ref[...] = ins[0][kept]
        a_ref[...] = ins[1][kept]
    for i, ref in enumerate(kv_refs):
        k_ref[i] = ref[:, :HEAD_DIM]
        v_ref[i, :, :HEAD_DIM] = ref[:, HEAD_DIM:]
        v_ref[i, :, HEAD_DIM:] = jnp.ones((ref.shape[0], HEAD_DIM), BF16)
    sub, chunk = 128, 1024
    steps = a_ref.shape[0] // chunk

    def part(t, nothing):
        piece, base = t // steps, t % steps * chunk

        def rows(r, start=0):
            return pl.ds(pl.multiple_of(base + r, sub) + start, sub)

        def scores(r):
            return lax.dot_general(
                q_ref[rows(r, offset)], k_ref[piece], (((1,), (1,)), ((), ())), preferred_element_type=F32
            )

        following = scores(0)
        for r in range(0, chunk, sub):
            s = following
            if r + sub < chunk:
                following = scores(r + sub)
            old = m_ref[rows(r), :1]
            best = jnp.maximum(jnp.max(s, axis=1, keepdims=True), old)
            weights = jnp.exp2(s - best).astype(BF16)
            acc = jnp.dot(weights, v_ref[piece], preferred_element_type=F32)
            acc = acc + a_ref[rows(r)] * jnp.exp2(old - best)
            m_ref[rows(r)] = jnp.broadcast_to(best, (sub, HEAD_DIM))
            a_ref[rows(r)] = acc
        return nothing

    if steps * pieces == 1:
        part(0, 0)
    else:
        lax.fori_loop(0, steps * pieces, part, 0)
    if last:
        lane = lax.broadcasted_iota(jnp.int32, m_ref.shape, 1)
        out_ref[:, :HEAD_DIM] = a_ref[:, :HEAD_DIM]
        out_ref[:, HEAD_DIM:] = jnp.where(lane < 64, a_ref[:, HEAD_DIM:], m_ref[...])


def attend(q, kvs, carry, last=None):
    first, count = carry is None, kvs[0].shape[0]
    rows = q.shape[0] // (1 if last is None else 2)
    shapes = [jax.ShapeDtypeStruct((rows, n), F32) for n in ((HEAD_DIM, 2 * HEAD_DIM) if last is None else (2 * HEAD_DIM,))]
    pieces = len(kvs)
    out = pl.pallas_call(
        functools.partial(attend_kernel, pieces=pieces, first=first, last=last is not None, offset=(last or 0) * rows),
        in_specs=[WHOLE] * (1 + pieces + (0 if first else 2)),
        out_specs=[WHOLE] * len(shapes),
        out_shape=shapes,
        scratch_shapes=([] if last is None else [pltpu.VMEM((rows, HEAD_DIM), F32), pltpu.VMEM((rows, 2 * HEAD_DIM), F32)])
        + [
            pltpu.VMEM((pieces, count, HEAD_DIM), BF16),
            pltpu.VMEM((pieces, count, 2 * HEAD_DIM), BF16),
        ],
        input_output_aliases={} if first or last is not None else {1 + pieces: 0, 2 + pieces: 1},
        compiler_params=pltpu.CompilerParams(vmem_limit_bytes=40 * 2**20),
        cost_estimate=pl.CostEstimate(
            flops=8 * rows * count * HEAD_DIM * pieces, bytes_accessed=8 * 2**20, transcendentals=rows * count
        ),
        name="attend",
    )(q, *kvs, *([] if first else carry))
    return out if last is None else out[0]


def project_out_kernel(i_ref, own_ref, got_ref, column, rest, rest_got, out_ref, w_ref, at_ref):
    fill_rows(i_ref, w_ref, column, rest, rest_got)
    rows = own_ref.shape[0] // GROUP
    for h in range(GROUP):
        mine, theirs = own_ref[h * rows : (h + 1) * rows], got_ref[h * rows : (h + 1) * rows]
        best_a, best_b = mine[:, 255:256], theirs[:, 255:256]
        top = jnp.maximum(best_a, best_b)
        both = mine * jnp.exp2(best_a - top) + theirs * jnp.exp2(best_b - top)
        at_ref[:, h * HEAD_DIM : (h + 1) * HEAD_DIM] = (both[:, :HEAD_DIM] / both[:, HEAD_DIM : HEAD_DIM + 1]).astype(BF16)
    out_ref[...] = lax.dot_general(
        at_ref[...], w_ref[...], (((1,), (1,)), ((), ())), preferred_element_type=F32
    ).astype(BF16)


def tables(positions):
    lane = jnp.arange(HEAD_DIM)
    f = lane % 32
    inverse_rate = rope_base ** (-(2 * f).astype(F32) / 64)
    row = (positions // GRID_W).astype(F32)
    column = (positions % GRID_W).astype(F32)
    place = jnp.where(lane[None] < 64, row[:, None], column[:, None])
    angle = place * inverse_rate[None]
    return jnp.cos(angle), jnp.sin(angle) * jnp.where((lane // 32) % 2 == 0, -1.0, 1.0)


def from_x(column, half):
    rest = jnp.concatenate([turn(column, X, NX), shift(half, X, NX, 2)], axis=0)
    return column, rest, other_core(rest)


def local(tokens, query_weight, key_weight, value_weight, out_weight, query_gain, key_gain):
    where = jnp.stack([lax.axis_index(a) for a in (Z, X, C, Y)]).astype(jnp.int32)
    rows = tokens.shape[0] * NY
    positions = lax.axis_index(SP) * rows + jnp.arange(rows, dtype=jnp.int32)
    cosine, sine = tables(positions)
    gain_q, gain_k = query_gain[None], key_gain[None]

    kv_weight = everyone(jnp.concatenate([key_weight, value_weight], axis=1), (Z, X))
    w_own = jnp.concatenate([query_weight, out_weight.T], axis=1)
    w_other = other_core(w_own)
    slab = jnp.concatenate([w_own, w_other], axis=0)
    leaps = leap(slab, 1), leap(slab, 2), leap(slab, 3), leap(w_own, 4)
    toks = [tokens] + [shift(tokens, Y, NY, -by) for by in (1, 2, 3)]
    kv_got = other_core(kv_weight)

    kv_own, rows_in = call(
        kv_kernel, [((rows, 256), BF16), ((rows, tokens.shape[1]), BF16)],
        where, *toks, kv_weight, kv_got, gain_k, cosine, sine,
        scratch=[pltpu.VMEM((tokens.shape[1], 256), BF16)],
    )
    mine = jnp.concatenate(after(leaps, kv_own), axis=0)
    got = other_core(mine)
    q_column, q_half, wo_column, wo_half = call(
        column_kernel, [((512, 512), BF16), ((256, 512), BF16)] * 2, where, w_own, w_other, mine, got,
    )
    kv_slab = jnp.concatenate([kv_own, other_core(kv_own)], axis=0)
    kv_near, kv_far = turn(kv_slab, X, NX), shift(kv_own, X, NX, 2)
    plane = jnp.concatenate([kv_own, kv_near, kv_far], axis=0)

    (q_own,) = call(
        q_kernel, [((GROUP * rows, HEAD_DIM), BF16)],
        where, rows_in, *from_x(q_column, q_half), gain_q, cosine, sine,
        scratch=[pltpu.VMEM((tokens.shape[1], 512), BF16)],
    )
    q_all = jnp.concatenate([q_own, other_core(q_own)], axis=0)
    wo_all = from_x(*after((wo_column, wo_half), q_own))

    chain = {"a": plane, "b": other_core(plane)}
    carry, todo = None, [plane]
    for step in range(1, 5):
        for name in "ab" if step < 4 else "a":
            chain[name] = turn(chain[name], Z, NZ)
            todo.append(chain[name])
    for at_once in (todo[0:2], todo[2:4], todo[4:6]):
        carry = attend(q_all, at_once, carry)
    theirs = attend(q_all, todo[6:], carry, last=1)
    got = other_core(theirs)
    own = attend(q_all, todo[6:], carry, last=0)
    (partial,) = call(
        project_out_kernel, [((rows, tokens.shape[1]), BF16)], where, own, got, *wo_all,
        scratch=[pltpu.VMEM((2048, 512), BF16), pltpu.VMEM((rows, GROUP * HEAD_DIM), BF16)],
    )
    pieces = partial.reshape(NY, -1, partial.shape[1])
    summed = jnp.sum(lax.all_to_all(pieces, Y, 0, 0).astype(F32), axis=0)
    mixed = summed * lax.rsqrt(jnp.mean(summed * summed, axis=-1, keepdims=True) + eps)
    return mixed.astype(BF16)


def solution(mesh):
    split = Mesh(mesh.devices.reshape(NZ, NX, NC, NY), SP_TP)

    return jax.shard_map(
        local,
        mesh=split,
        in_specs=(P(SP_TP, None), P(SP, Y), P(SP, Y), P(SP, Y), P(Y, SP), P(), P()),
        out_specs=P(SP_TP, None),
        check_vma=False,
    )
```

```python
import functools
import math

import jax
import jax.numpy as jnp
from jax import lax
from jax.experimental import pallas as pl
from jax.experimental.pallas import tpu as pltpu
from jax.sharding import Mesh
from jax.sharding import PartitionSpec as P


HEAD_DIM = 128
GROUP = 4
GRID_W = 64
Z, X, C, Y = "sp_0", "sp_1", "sp_2", "tp"
SP = (Z, X, C)
SP_TP = (Z, X, C, Y)
NZ, NX, NC, NY = 8, 4, 2, 4

eps = 1e-06
rope_base = 10000.0

F32 = jnp.float32
BF16 = jnp.bfloat16
WHOLE = pl.BlockSpec(memory_space=pltpu.VMEM)
SCALARS = pl.BlockSpec(memory_space=pltpu.SMEM)


def other_core(piece):
    return lax.ppermute(piece, C, [(0, 1), (1, 0)])


def turn(piece, axis, count):
    pairs = []
    for i in range(count):
        pairs += [(i * 2, (i + 1) % count * 2), (i * 2 + 1, (i - 1) % count * 2 + 1)]
    return lax.ppermute(piece, (axis, C), pairs)


def shift(piece, axis, count, by):
    return lax.ppermute(piece, axis, [(i, (i + by) % count) for i in range(count)])


def leap(piece, by):
    pairs = []
    for i in range(NZ):
        pairs += [(i * 2, (i + by) % NZ * 2), (i * 2 + 1, (i - by) % NZ * 2 + 1)]
    return lax.ppermute(piece, (Z, C), pairs)


def everyone(piece, axes):
    n = lax.axis_size(axes)
    return lax.all_to_all(jnp.broadcast_to(piece[None], (n,) + piece.shape), axes, 0, 0)


def after(value, *events):
    return lax.optimization_barrier((value, *events))[0]


def call(kernel, outs, *args, scratch=(), flops=0):
    return pl.pallas_call(
        kernel,
        in_specs=[SCALARS] + [WHOLE] * (len(args) - 1),
        out_specs=[WHOLE] * len(outs),
        out_shape=[jax.ShapeDtypeStruct(s, d) for s, d in outs],
        scratch_shapes=list(scratch),
        compiler_params=pltpu.CompilerParams(vmem_limit_bytes=40 * 2**20),
        cost_estimate=pl.CostEstimate(flops=flops, bytes_accessed=4 * 2**20, transcendentals=0),
    )(*args)


def at(index, size):
    return pl.ds(pl.multiple_of(index * size, size), size)


def column_kernel(i_ref, own_ref, other_ref, mine_ref, got_ref, q_ref, q_half_ref, o_ref, o_half_ref):
    z, c = i_ref[0], i_ref[2]
    away = 1 - 2 * c
    width = q_ref.shape[1]

    def put(ref, start, plane, half):
        place = at(half * NZ + (plane + 2 * NZ) % NZ, 32)
        q_ref[place, :] = ref[start : start + 32, :width]
        o_ref[place, :] = ref[start : start + 32, width:]

    put(own_ref, 0, z, c)
    put(other_ref, 0, z, 1 - c)
    for s in range(1, 4):
        for j in range(2):
            half = jnp.where(c == 0, j, 1 - j)
            start = s * 64 - 64 + j * 32
            put(mine_ref, start, z - away * s, half)
            put(got_ref, start, z + away * s, 1 - half)
    put(mine_ref, 192, z + 4, c)
    put(got_ref, 192, z + 4, 1 - c)
    q_half_ref[...] = q_ref[at(c, 256), :]
    o_half_ref[...] = o_ref[at(c, 256), :]


def join_kernel(i_ref, near_ref, far_ref, out_ref):
    out_ref[:512, :] = near_ref[...]
    out_ref[512:, :] = far_ref[...]


def fill_rows(i_ref, w_ref, column, rest, got):
    x, c = i_ref[1], i_ref[2]
    minus = (x + jnp.where(c == 0, 3, 1)) % NX
    plus = (x + jnp.where(c == 0, 1, 3)) % NX
    opposite = (x + 2) % NX

    def plane(z, nothing):
        row = pl.multiple_of(z * 32, 32)
        for k in range(2):
            place = pl.ds(row + k * 256, 32)
            for ref, where in ((column, x), (rest, minus), (got, plus)):
                w_ref[at((z * NX + where) * 2 + k, 32), :] = ref[place, :]
        w_ref[at((z * NX + opposite) * 2 + c, 32), :] = rest[pl.ds(row + 512, 32), :]
        w_ref[at((z * NX + opposite) * 2 + 1 - c, 32), :] = got[pl.ds(row + 512, 32), :]
        return nothing

    lax.fori_loop(0, NZ, plane, 0)


def rotated(raw, gain, cosine, sine, scale):
    wide = raw.astype(F32)
    n = wide * lax.rsqrt(jnp.mean(wide * wide, axis=-1, keepdims=True) + eps) * gain
    lane = lax.broadcasted_iota(jnp.int32, n.shape, 1)
    swapped = jnp.where(lane // 32 % 2 == 0, pltpu.roll(n, 96, 1), pltpu.roll(n, 32, 1))
    return ((n * cosine + swapped * sine) * scale).astype(BF16)


def kv_kernel(i_ref, t0, t1, t2, t3, own, got, gain, cosine, sine, kv_ref, t_ref, w_ref):
    c, y = i_ref[2], i_ref[3]
    for by, ref in enumerate((t0, t1, t2, t3)):
        t_ref[at((y + by) % NY, 64), :] = ref[...]

    def chip(i, nothing):
        for k in range(4):
            w_ref[at((i * 4 + k) * 2 + c, 32), :] = own[i * 4 + k]
            w_ref[at((i * 4 + k) * 2 + 1 - c, 32), :] = got[i * 4 + k]
        return nothing

    lax.fori_loop(0, NZ * NX // 4, chip, 0)
    raw = jnp.dot(t_ref[...], w_ref[...], preferred_element_type=F32).astype(BF16)
    kv_ref[:, :HEAD_DIM] = rotated(raw[:, :HEAD_DIM], gain[...], cosine[...], sine[...], 1.0)
    kv_ref[:, HEAD_DIM:] = raw[:, HEAD_DIM:]


def q_kernel(i_ref, t_ref, column, rest, got, gain, cosine, sine, q_ref, w_ref):
    fill_rows(i_ref, w_ref, column, rest, got)
    raw = jnp.dot(t_ref[...], w_ref[...], preferred_element_type=F32).astype(BF16)
    rows = raw.shape[0]
    scale = HEAD_DIM ** (-0.5) * math.log2(math.e)
    for h in range(GROUP):
        head = raw[:, h * HEAD_DIM : (h + 1) * HEAD_DIM]
        q_ref[h * rows : (h + 1) * rows, :] = rotated(head, gain[...], cosine[...], sine[...], scale)


def attend_kernel(*refs, pieces, first, last, offset):
    q_ref, *kv_refs = refs[: 1 + pieces]
    ins = refs[1 + pieces : 1 + pieces + (0 if first else 2)]
    *outs, k_ref, v_ref = refs[1 + pieces + len(ins) :]
    out_ref, m_ref, a_ref = outs if last else (None, *outs)
    if first:
        m_ref[...] = jnp.full(m_ref.shape, -1e30, F32)
        a_ref[...] = jnp.zeros(a_ref.shape, F32)
    else:
        kept = slice(offset, offset + m_ref.shape[0])
        m_ref[...] = ins[0][kept]
        a_ref[...] = ins[1][kept]
    for i, ref in enumerate(kv_refs):
        k_ref[i] = ref[:, :HEAD_DIM]
        v_ref[i, :, :HEAD_DIM] = ref[:, HEAD_DIM:]
        v_ref[i, :, HEAD_DIM:] = jnp.ones((ref.shape[0], HEAD_DIM), BF16)
    sub, chunk = 128, 1024
    steps = a_ref.shape[0] // chunk

    def part(t, nothing):
        piece, base = t // steps, t % steps * chunk

        def rows(r, start=0):
            return pl.ds(pl.multiple_of(base + r, sub) + start, sub)

        def scores(r):
            return lax.dot_general(
                q_ref[rows(r, offset)], k_ref[piece], (((1,), (1,)), ((), ())), preferred_element_type=F32
            )

        following = scores(0)
        for r in range(0, chunk, sub):
            s = following
            if r + sub < chunk:
                following = scores(r + sub)
            old = m_ref[rows(r), :1]
            best = jnp.maximum(jnp.max(s, axis=1, keepdims=True), old)
            weights = jnp.exp2(s - best).astype(BF16)
            acc = jnp.dot(weights, v_ref[piece], preferred_element_type=F32)
            acc = acc + a_ref[rows(r)] * jnp.exp2(old - best)
            m_ref[rows(r)] = jnp.broadcast_to(best, (sub, HEAD_DIM))
            a_ref[rows(r)] = acc
        return nothing

    if steps * pieces == 1:
        part(0, 0)
    else:
        lax.fori_loop(0, steps * pieces, part, 0)
    if last:
        lane = lax.broadcasted_iota(jnp.int32, m_ref.shape, 1)
        out_ref[:, :HEAD_DIM] = a_ref[:, :HEAD_DIM]
        out_ref[:, HEAD_DIM:] = jnp.where(lane < 64, a_ref[:, HEAD_DIM:], m_ref[...])


def attend(q, kvs, carry, last=None):
    first, count = carry is None, kvs[0].shape[0]
    rows = q.shape[0] // (1 if last is None else 2)
    shapes = [jax.ShapeDtypeStruct((rows, n), F32) for n in ((HEAD_DIM, 2 * HEAD_DIM) if last is None else (2 * HEAD_DIM,))]
    pieces = len(kvs)
    out = pl.pallas_call(
        functools.partial(attend_kernel, pieces=pieces, first=first, last=last is not None, offset=(last or 0) * rows),
        in_specs=[WHOLE] * (1 + pieces + (0 if first else 2)),
        out_specs=[WHOLE] * len(shapes),
        out_shape=shapes,
        scratch_shapes=([] if last is None else [pltpu.VMEM((rows, HEAD_DIM), F32), pltpu.VMEM((rows, 2 * HEAD_DIM), F32)])
        + [
            pltpu.VMEM((pieces, count, HEAD_DIM), BF16),
            pltpu.VMEM((pieces, count, 2 * HEAD_DIM), BF16),
        ],
        input_output_aliases={} if first or last is not None else {1 + pieces: 0, 2 + pieces: 1},
        compiler_params=pltpu.CompilerParams(vmem_limit_bytes=40 * 2**20),
        cost_estimate=pl.CostEstimate(
            flops=8 * rows * count * HEAD_DIM * pieces, bytes_accessed=8 * 2**20, transcendentals=rows * count
        ),
        name="attend",
    )(q, *kvs, *([] if first else carry))
    return out if last is None else out[0]


def project_out_kernel(i_ref, own_ref, got_ref, column, rest, rest_got, out_ref, w_ref, at_ref):
    fill_rows(i_ref, w_ref, column, rest, rest_got)
    rows = own_ref.shape[0] // GROUP
    for h in range(GROUP):
        mine, theirs = own_ref[h * rows : (h + 1) * rows], got_ref[h * rows : (h + 1) * rows]
        best_a, best_b = mine[:, 255:256], theirs[:, 255:256]
        top = jnp.maximum(best_a, best_b)
        both = mine * jnp.exp2(best_a - top) + theirs * jnp.exp2(best_b - top)
        at_ref[:, h * HEAD_DIM : (h + 1) * HEAD_DIM] = (both[:, :HEAD_DIM] / both[:, HEAD_DIM : HEAD_DIM + 1]).astype(BF16)
    out_ref[...] = lax.dot_general(
        at_ref[...], w_ref[...], (((1,), (1,)), ((), ())), preferred_element_type=F32
    ).astype(BF16)


def tables(positions):
    lane = jnp.arange(HEAD_DIM)
    f = lane % 32
    inverse_rate = rope_base ** (-(2 * f).astype(F32) / 64)
    row = (positions // GRID_W).astype(F32)
    column = (positions % GRID_W).astype(F32)
    place = jnp.where(lane[None] < 64, row[:, None], column[:, None])
    angle = place * inverse_rate[None]
    return jnp.cos(angle), jnp.sin(angle) * jnp.where((lane // 32) % 2 == 0, -1.0, 1.0)


def start_x(column, half):
    return column, turn(column, X, NX), shift(half, X, NX, 2)


def finish_x(where, column, near, far):
    (rest,) = call(join_kernel, [((768, near.shape[1]), BF16)], where, near, far)
    return column, rest, other_core(rest)


def local(tokens, query_weight, key_weight, value_weight, out_weight, query_gain, key_gain):
    where = jnp.stack([lax.axis_index(a) for a in (Z, X, C, Y)]).astype(jnp.int32)
    rows = tokens.shape[0] * NY
    positions = lax.axis_index(SP) * rows + jnp.arange(rows, dtype=jnp.int32)
    cosine, sine = tables(positions)
    gain_q, gain_k = query_gain[None], key_gain[None]

    kv_weight = everyone(jnp.concatenate([key_weight, value_weight], axis=1), (Z, X))
    w_own = jnp.concatenate([query_weight, out_weight.T], axis=1)
    w_other = other_core(w_own)
    slab = jnp.concatenate([w_own, w_other], axis=0)
    leaps = leap(slab, 1), leap(slab, 2), leap(slab, 3)
    leaps += (leap(w_own, 4),)
    toks = [tokens] + [shift(tokens, Y, NY, -by) for by in (1, 2, 3)]
    kv_got = other_core(kv_weight)

    kv_own, rows_in = call(
        kv_kernel, [((rows, 256), BF16), ((rows, tokens.shape[1]), BF16)],
        where, *toks, kv_weight, kv_got, gain_k, cosine, sine,
        scratch=[pltpu.VMEM((tokens.shape[1], 256), BF16)],
    )
    mine = jnp.concatenate(after(leaps, kv_own), axis=0)
    got = other_core(mine)
    q_column, q_half, wo_column, wo_half = call(
        column_kernel, [((512, 512), BF16), ((256, 512), BF16)] * 2, where, w_own, w_other, mine, got,
    )
    parts = [shift(kv_own, X, NX, by) for by in (2, 1, 3)]
    plane = jnp.concatenate([kv_own, *parts], axis=0)

    (q_own,) = call(
        q_kernel, [((GROUP * rows, HEAD_DIM), BF16)],
        where, rows_in, *finish_x(where, *start_x(q_column, q_half)), gain_q, cosine, sine,
        scratch=[pltpu.VMEM((tokens.shape[1], 512), BF16)],
    )
    q_all = jnp.concatenate([q_own, other_core(q_own)], axis=0)
    wo_column, *wo_parts = start_x(wo_column, wo_half)

    chain = {"a": plane, "b": other_core(plane)}
    carry, todo = None, [plane]
    for step in range(1, 5):
        for name in "ab" if step < 4 else "a":
            chain[name] = turn(chain[name], Z, NZ)
            todo.append(chain[name])
    for i, at_once in enumerate((todo[0:2], todo[2:4], todo[4:6])):
        carry = attend(q_all, at_once, carry)
        if i == 1:
            wo_all = finish_x(where, wo_column, *wo_parts)
    theirs = attend(q_all, todo[6:], carry, last=1)
    got = other_core(theirs)
    own = attend(q_all, todo[6:], carry, last=0)
    (partial,) = call(
        project_out_kernel, [((rows, tokens.shape[1]), BF16)], where, own, got, *wo_all,
        scratch=[pltpu.VMEM((2048, 512), BF16), pltpu.VMEM((rows, GROUP * HEAD_DIM), BF16)],
    )
    pieces = partial.reshape(NY, -1, partial.shape[1])
    summed = jnp.sum(lax.all_to_all(pieces, Y, 0, 0).astype(F32), axis=0)
    mixed = summed * lax.rsqrt(jnp.mean(summed * summed, axis=-1, keepdims=True) + eps)
    return mixed.astype(BF16)


def solution(mesh):
    split = Mesh(mesh.devices.reshape(NZ, NX, NC, NY), SP_TP)

    return jax.shard_map(
        local,
        mesh=split,
        in_specs=(P(SP_TP, None), P(SP, Y), P(SP, Y), P(SP, Y), P(Y, SP), P(), P()),
        out_specs=P(SP_TP, None),
        check_vma=False,
    )
```

```python
import functools
import math

import jax
import jax.numpy as jnp
from jax import lax
from jax.experimental import pallas as pl
from jax.experimental.pallas import tpu as pltpu
from jax.sharding import Mesh
from jax.sharding import PartitionSpec as P


HEAD_DIM = 128
GROUP = 4
GRID_W = 64
Z, X, C, Y = "sp_0", "sp_1", "sp_2", "tp"
SP = (Z, X, C)
SP_TP = (Z, X, C, Y)
NZ, NX, NC, NY = 8, 4, 2, 4

eps = 1e-06
rope_base = 10000.0

F32 = jnp.float32
BF16 = jnp.bfloat16
WHOLE = pl.BlockSpec(memory_space=pltpu.VMEM)
SCALARS = pl.BlockSpec(memory_space=pltpu.SMEM)


def other_core(piece):
    return lax.ppermute(piece, C, [(0, 1), (1, 0)])


def turn(piece, axis, count):
    pairs = []
    for i in range(count):
        pairs += [(i * 2, (i + 1) % count * 2), (i * 2 + 1, (i - 1) % count * 2 + 1)]
    return lax.ppermute(piece, (axis, C), pairs)


def shift(piece, axis, count, by):
    return lax.ppermute(piece, axis, [(i, (i + by) % count) for i in range(count)])


def leap(piece, by):
    pairs = []
    for i in range(NZ):
        pairs += [(i * 2, (i + by) % NZ * 2), (i * 2 + 1, (i - by) % NZ * 2 + 1)]
    return lax.ppermute(piece, (Z, C), pairs)


def everyone(piece, axes):
    n = lax.axis_size(axes)
    return lax.all_to_all(jnp.broadcast_to(piece[None], (n,) + piece.shape), axes, 0, 0)


def after(value, *events):
    return lax.optimization_barrier((value, *events))[0]


def call(kernel, outs, *args, scratch=(), flops=0):
    return pl.pallas_call(
        kernel,
        in_specs=[SCALARS] + [WHOLE] * (len(args) - 1),
        out_specs=[WHOLE] * len(outs),
        out_shape=[jax.ShapeDtypeStruct(s, d) for s, d in outs],
        scratch_shapes=list(scratch),
        compiler_params=pltpu.CompilerParams(vmem_limit_bytes=40 * 2**20),
        cost_estimate=pl.CostEstimate(flops=flops, bytes_accessed=4 * 2**20, transcendentals=0),
    )(*args)


def at(index, size):
    return pl.ds(pl.multiple_of(index * size, size), size)


def column_kernel(i_ref, own_ref, other_ref, mine_ref, got_ref, q_ref, q_half_ref, o_ref, o_half_ref):
    z, c = i_ref[0], i_ref[2]
    away = 1 - 2 * c
    width = q_ref.shape[1]

    def put(ref, start, plane, half):
        place = at(half * NZ + (plane + 2 * NZ) % NZ, 32)
        q_ref[place, :] = ref[start : start + 32, :width]
        o_ref[place, :] = ref[start : start + 32, width:]

    put(own_ref, 0, z, c)
    put(other_ref, 0, z, 1 - c)
    for s in range(1, 4):
        for j in range(2):
            half = jnp.where(c == 0, j, 1 - j)
            start = s * 64 - 64 + j * 32
            put(mine_ref, start, z - away * s, half)
            put(got_ref, start, z + away * s, 1 - half)
    put(mine_ref, 192, z + 4, c)
    put(got_ref, 192, z + 4, 1 - c)
    q_half_ref[...] = q_ref[at(c, 256), :]
    o_half_ref[...] = o_ref[at(c, 256), :]


def join_kernel(i_ref, near_ref, far_ref, out_ref):
    out_ref[:512, :] = near_ref[...]
    out_ref[512:, :] = far_ref[...]


def fill_rows(i_ref, w_ref, column, rest, got):
    x, c = i_ref[1], i_ref[2]
    minus = (x + jnp.where(c == 0, 3, 1)) % NX
    plus = (x + jnp.where(c == 0, 1, 3)) % NX
    opposite = (x + 2) % NX

    def plane(z, nothing):
        row = pl.multiple_of(z * 32, 32)
        for k in range(2):
            place = pl.ds(row + k * 256, 32)
            for ref, where in ((column, x), (rest, minus), (got, plus)):
                w_ref[at((z * NX + where) * 2 + k, 32), :] = ref[place, :]
        w_ref[at((z * NX + opposite) * 2 + c, 32), :] = rest[pl.ds(row + 512, 32), :]
        w_ref[at((z * NX + opposite) * 2 + 1 - c, 32), :] = got[pl.ds(row + 512, 32), :]
        return nothing

    lax.fori_loop(0, NZ, plane, 0)


def rotated(raw, gain, cosine, sine, scale):
    wide = raw.astype(F32)
    n = wide * lax.rsqrt(jnp.mean(wide * wide, axis=-1, keepdims=True) + eps) * gain
    lane = lax.broadcasted_iota(jnp.int32, n.shape, 1)
    swapped = jnp.where(lane // 32 % 2 == 0, pltpu.roll(n, 96, 1), pltpu.roll(n, 32, 1))
    return ((n * cosine + swapped * sine) * scale).astype(BF16)


def kv_kernel(i_ref, t0, t1, t2, t3, own, got, gain, cosine, sine, kv_ref, t_ref, w_ref):
    c, y = i_ref[2], i_ref[3]
    for by, ref in enumerate((t0, t1, t2, t3)):
        t_ref[at((y + by) % NY, 64), :] = ref[...]

    def chip(i, nothing):
        for k in range(4):
            w_ref[at((i * 4 + k) * 2 + c, 32), :] = own[i * 4 + k]
            w_ref[at((i * 4 + k) * 2 + 1 - c, 32), :] = got[i * 4 + k]
        return nothing

    lax.fori_loop(0, NZ * NX // 4, chip, 0)
    raw = jnp.dot(t_ref[...], w_ref[...], preferred_element_type=F32).astype(BF16)
    kv_ref[:, :HEAD_DIM] = rotated(raw[:, :HEAD_DIM], gain[...], cosine[...], sine[...], 1.0)
    kv_ref[:, HEAD_DIM:] = raw[:, HEAD_DIM:]


def q_kernel(i_ref, t_ref, column, rest, got, gain, cosine, sine, q_ref, w_ref):
    fill_rows(i_ref, w_ref, column, rest, got)
    raw = jnp.dot(t_ref[...], w_ref[...], preferred_element_type=F32).astype(BF16)
    rows = raw.shape[0]
    scale = HEAD_DIM ** (-0.5) * math.log2(math.e)
    for h in range(GROUP):
        head = raw[:, h * HEAD_DIM : (h + 1) * HEAD_DIM]
        q_ref[h * rows : (h + 1) * rows, :] = rotated(head, gain[...], cosine[...], sine[...], scale)


def attend_kernel(*refs, pieces, first, last, offset):
    q_ref, *kv_refs = refs[: 1 + pieces]
    ins = refs[1 + pieces : 1 + pieces + (0 if first else 2)]
    *outs, k_ref, v_ref = refs[1 + pieces + len(ins) :]
    for i, ref in enumerate(kv_refs):
        keys = slice(i * ref.shape[0], (i + 1) * ref.shape[0])
        k_ref[:, keys] = ref[:, :HEAD_DIM].T
        v_ref[keys, :HEAD_DIM] = ref[:, HEAD_DIM:]
    v_ref[:, HEAD_DIM:] = jnp.ones((v_ref.shape[0], HEAD_DIM), BF16)
    sub, chunk = 128, 512
    lane = lax.broadcasted_iota(jnp.int32, (sub, HEAD_DIM), 1)

    def part(t, nothing):
        def rows(r, start=0):
            return pl.ds(pl.multiple_of(t * chunk + r, sub) + start, sub)

        def scores(r):
            return jnp.dot(q_ref[rows(r, offset)], k_ref[...], preferred_element_type=F32)

        following = scores(0)
        for r in range(0, chunk, sub):
            s = following
            if r + sub < chunk:
                following = scores(r + sub)
            best = jnp.max(s, axis=1, keepdims=True)
            if not first:
                old = ins[0][rows(r, offset), :1]
                best = jnp.maximum(best, old)
            weights = jnp.exp2(s - best).astype(BF16)
            acc = jnp.dot(weights, v_ref[...], preferred_element_type=F32)
            if not first:
                acc = acc + ins[1][rows(r, offset)] * jnp.exp2(old - best)
            if last:
                outs[0][rows(r), :HEAD_DIM] = acc[:, :HEAD_DIM]
                outs[0][rows(r), HEAD_DIM:] = jnp.where(lane < 64, acc[:, HEAD_DIM:], best)
            else:
                outs[0][rows(r)] = jnp.broadcast_to(best, (sub, HEAD_DIM))
                outs[1][rows(r)] = acc
        return nothing

    lax.fori_loop(0, outs[0].shape[0] // chunk, part, 0)


def attend(q, kvs, carry, last=None):
    first, count = carry is None, kvs[0].shape[0]
    rows = q.shape[0] // (1 if last is None else 2)
    shapes = [jax.ShapeDtypeStruct((rows, n), F32) for n in ((HEAD_DIM, 2 * HEAD_DIM) if last is None else (2 * HEAD_DIM,))]
    pieces = len(kvs)
    out = pl.pallas_call(
        functools.partial(attend_kernel, pieces=pieces, first=first, last=last is not None, offset=(last or 0) * rows),
        in_specs=[WHOLE] * (1 + pieces + (0 if first else 2)),
        out_specs=[WHOLE] * len(shapes),
        out_shape=shapes,
        scratch_shapes=[
            pltpu.VMEM((HEAD_DIM, pieces * count), BF16),
            pltpu.VMEM((pieces * count, 2 * HEAD_DIM), BF16),
        ],
        input_output_aliases={} if first or last is not None else {1 + pieces: 0, 2 + pieces: 1},
        compiler_params=pltpu.CompilerParams(vmem_limit_bytes=40 * 2**20),
        cost_estimate=pl.CostEstimate(
            flops=8 * rows * count * HEAD_DIM * pieces, bytes_accessed=8 * 2**20, transcendentals=rows * count
        ),
        name="attend",
    )(q, *kvs, *([] if first else carry))
    return out if last is None else out[0]


def project_out_kernel(i_ref, own_ref, got_ref, column, rest, rest_got, out_ref, w_ref, at_ref):
    fill_rows(i_ref, w_ref, column, rest, rest_got)
    rows = own_ref.shape[0] // GROUP
    for h in range(GROUP):
        mine, theirs = own_ref[h * rows : (h + 1) * rows], got_ref[h * rows : (h + 1) * rows]
        best_a, best_b = mine[:, 255:256], theirs[:, 255:256]
        top = jnp.maximum(best_a, best_b)
        both = mine * jnp.exp2(best_a - top) + theirs * jnp.exp2(best_b - top)
        at_ref[:, h * HEAD_DIM : (h + 1) * HEAD_DIM] = (both[:, :HEAD_DIM] / both[:, HEAD_DIM : HEAD_DIM + 1]).astype(BF16)
    out_ref[...] = lax.dot_general(
        at_ref[...], w_ref[...], (((1,), (1,)), ((), ())), preferred_element_type=F32
    ).astype(BF16)


def tables(positions):
    lane = jnp.arange(HEAD_DIM)
    f = lane % 32
    inverse_rate = rope_base ** (-(2 * f).astype(F32) / 64)
    row = (positions // GRID_W).astype(F32)
    column = (positions % GRID_W).astype(F32)
    place = jnp.where(lane[None] < 64, row[:, None], column[:, None])
    angle = place * inverse_rate[None]
    return jnp.cos(angle), jnp.sin(angle) * jnp.where((lane // 32) % 2 == 0, -1.0, 1.0)


def start_x(column, half):
    near = turn(column, X, NX)
    return column, near, shift(half, X, NX, 2)


def finish_x(where, column, near, far):
    (rest,) = call(join_kernel, [((768, near.shape[1]), BF16)], where, near, far)
    return column, rest, other_core(rest)


def local(tokens, query_weight, key_weight, value_weight, out_weight, query_gain, key_gain):
    where = jnp.stack([lax.axis_index(a) for a in (Z, X, C, Y)]).astype(jnp.int32)
    rows = tokens.shape[0] * NY
    positions = lax.axis_index(SP) * rows + jnp.arange(rows, dtype=jnp.int32)
    cosine, sine = tables(positions)
    gain_q, gain_k = query_gain[None], key_gain[None]

    kv_weight = everyone(jnp.concatenate([key_weight, value_weight], axis=1), (Z, X))
    w_own = jnp.concatenate([query_weight, out_weight.T], axis=1)
    w_other = other_core(w_own)
    slab = jnp.concatenate([w_own, w_other], axis=0)
    leaps = leap(slab, 1), leap(slab, 2), leap(slab, 3)
    leaps += (leap(w_own, 4),)
    toks = [tokens] + [shift(tokens, Y, NY, -by) for by in (1, 2, 3)]
    kv_got = other_core(kv_weight)

    kv_own, rows_in = call(
        kv_kernel, [((rows, 256), BF16), ((rows, tokens.shape[1]), BF16)],
        where, *toks, kv_weight, kv_got, gain_k, cosine, sine,
        scratch=[pltpu.VMEM((tokens.shape[1], 256), BF16)],
    )
    mine = jnp.concatenate(after(leaps, kv_own), axis=0)
    got = other_core(mine)
    q_column, q_half, wo_column, wo_half = call(
        column_kernel, [((512, 512), BF16), ((256, 512), BF16)] * 2, where, w_own, w_other, mine, got,
    )
    parts = [shift(kv_own, X, NX, by) for by in (2, 1, 3)]
    plane = jnp.concatenate([kv_own, *parts], axis=0)

    (q_own,) = call(
        q_kernel, [((GROUP * rows, HEAD_DIM), BF16)],
        where, rows_in, *finish_x(where, *start_x(q_column, q_half)), gain_q, cosine, sine,
        scratch=[pltpu.VMEM((tokens.shape[1], 512), BF16)],
    )
    q_all = jnp.concatenate([q_own, other_core(q_own)], axis=0)
    wo_column, *wo_parts = start_x(wo_column, wo_half)

    chain = {"a": plane, "b": other_core(plane)}
    carry, todo = None, [plane]
    for step in range(1, 5):
        for name in "ab" if step < 4 else "a":
            chain[name] = turn(chain[name], Z, NZ)
            todo.append(chain[name])
    for i, at_once in enumerate((todo[0:2], todo[2:4], todo[4:6])):
        carry = attend(q_all, at_once, carry)
        if i == 1:
            wo_all = finish_x(where, wo_column, *wo_parts)
    theirs = attend(q_all, todo[6:], carry, last=1)
    got = other_core(theirs)
    own = attend(q_all, todo[6:], carry, last=0)
    (partial,) = call(
        project_out_kernel, [((rows, tokens.shape[1]), BF16)], where, own, got, *wo_all,
        scratch=[pltpu.VMEM((2048, 512), BF16), pltpu.VMEM((rows, GROUP * HEAD_DIM), BF16)],
    )
    pieces = partial.reshape(NY, -1, partial.shape[1])
    summed = jnp.sum(lax.all_to_all(pieces, Y, 0, 0).astype(F32), axis=0)
    mixed = summed * lax.rsqrt(jnp.mean(summed * summed, axis=-1, keepdims=True) + eps)
    return mixed.astype(BF16)


def solution(mesh):
    split = Mesh(mesh.devices.reshape(NZ, NX, NC, NY), SP_TP)

    return jax.shard_map(
        local,
        mesh=split,
        in_specs=(P(SP_TP, None), P(SP, Y), P(SP, Y), P(SP, Y), P(Y, SP), P(), P()),
        out_specs=P(SP_TP, None),
        check_vma=False,
    )
```

```python
import functools
import math

import jax
import jax.numpy as jnp
from jax import lax
from jax.experimental import pallas as pl
from jax.experimental.pallas import tpu as pltpu
from jax.sharding import Mesh
from jax.sharding import PartitionSpec as P


HEAD_DIM = 128
GROUP = 4
GRID_W = 64
Z, X, C, Y = "sp_0", "sp_1", "sp_2", "tp"
SP = (Z, X, C)
SP_TP = (Z, X, C, Y)
NZ, NX, NC, NY = 8, 4, 2, 4

eps = 1e-06
rope_base = 10000.0

F32 = jnp.float32
BF16 = jnp.bfloat16
WHOLE = pl.BlockSpec(memory_space=pltpu.VMEM)
SCALARS = pl.BlockSpec(memory_space=pltpu.SMEM)


def other_core(piece):
    return lax.ppermute(piece, C, [(0, 1), (1, 0)])


def turn(piece, axis, count):
    pairs = []
    for i in range(count):
        pairs += [(i * 2, (i + 1) % count * 2), (i * 2 + 1, (i - 1) % count * 2 + 1)]
    return lax.ppermute(piece, (axis, C), pairs)


def shift(piece, axis, count, by):
    return lax.ppermute(piece, axis, [(i, (i + by) % count) for i in range(count)])


def leap(piece, by):
    pairs = []
    for i in range(NZ):
        pairs += [(i * 2, (i + by) % NZ * 2), (i * 2 + 1, (i - by) % NZ * 2 + 1)]
    return lax.ppermute(piece, (Z, C), pairs)


def everyone(piece, axes):
    n = lax.axis_size(axes)
    return lax.all_to_all(jnp.broadcast_to(piece[None], (n,) + piece.shape), axes, 0, 0)


def after(value, *events):
    return lax.optimization_barrier((value, *events))[0]


def call(kernel, outs, *args, scratch=(), flops=0):
    return pl.pallas_call(
        kernel,
        in_specs=[SCALARS] + [WHOLE] * (len(args) - 1),
        out_specs=[WHOLE] * len(outs),
        out_shape=[jax.ShapeDtypeStruct(s, d) for s, d in outs],
        scratch_shapes=list(scratch),
        compiler_params=pltpu.CompilerParams(vmem_limit_bytes=40 * 2**20),
        cost_estimate=pl.CostEstimate(flops=flops, bytes_accessed=4 * 2**20, transcendentals=0),
    )(*args)


def at(index, size):
    return pl.ds(pl.multiple_of(index * size, size), size)


def column_kernel(i_ref, own_ref, other_ref, mine_ref, got_ref, q_ref, q_half_ref, o_ref, o_half_ref):
    z, c = i_ref[0], i_ref[2]
    away = 1 - 2 * c
    width = q_ref.shape[1]

    def put(ref, start, plane, half):
        place = at(half * NZ + (plane + 2 * NZ) % NZ, 32)
        q_ref[place, :] = ref[start : start + 32, :width]
        o_ref[place, :] = ref[start : start + 32, width:]

    put(own_ref, 0, z, c)
    put(other_ref, 0, z, 1 - c)
    for s in range(1, 4):
        for j in range(2):
            half = jnp.where(c == 0, j, 1 - j)
            start = s * 64 - 64 + j * 32
            put(mine_ref, start, z - away * s, half)
            put(got_ref, start, z + away * s, 1 - half)
    put(mine_ref, 192, z + 4, c)
    put(got_ref, 192, z + 4, 1 - c)
    q_half_ref[...] = q_ref[at(c, 256), :]
    o_half_ref[...] = o_ref[at(c, 256), :]


def join_kernel(i_ref, near_ref, far_ref, out_ref):
    out_ref[:512, :] = near_ref[...]
    out_ref[512:, :] = far_ref[...]


def fill_rows(i_ref, w_ref, column, rest, got):
    x, c = i_ref[1], i_ref[2]
    minus = (x + jnp.where(c == 0, 3, 1)) % NX
    plus = (x + jnp.where(c == 0, 1, 3)) % NX
    opposite = (x + 2) % NX

    def plane(z, nothing):
        row = pl.multiple_of(z * 32, 32)
        for k in range(2):
            place = pl.ds(row + k * 256, 32)
            for ref, where in ((column, x), (rest, minus), (got, plus)):
                w_ref[at((z * NX + where) * 2 + k, 32), :] = ref[place, :]
        w_ref[at((z * NX + opposite) * 2 + c, 32), :] = rest[pl.ds(row + 512, 32), :]
        w_ref[at((z * NX + opposite) * 2 + 1 - c, 32), :] = got[pl.ds(row + 512, 32), :]
        return nothing

    lax.fori_loop(0, NZ, plane, 0)


def rotated(raw, gain, cosine, sine, scale):
    wide = raw.astype(F32)
    n = wide * lax.rsqrt(jnp.mean(wide * wide, axis=-1, keepdims=True) + eps) * gain
    lane = lax.broadcasted_iota(jnp.int32, n.shape, 1)
    swapped = jnp.where(lane // 32 % 2 == 0, pltpu.roll(n, 96, 1), pltpu.roll(n, 32, 1))
    return ((n * cosine + swapped * sine) * scale).astype(BF16)


def kv_kernel(i_ref, t0, t1, t2, t3, own, got, gain, cosine, sine, kv_ref, t_ref, w_ref):
    c, y = i_ref[2], i_ref[3]
    for by, ref in enumerate((t0, t1, t2, t3)):
        t_ref[at((y + by) % NY, 64), :] = ref[...]

    def chip(i, nothing):
        for k in range(4):
            w_ref[at((i * 4 + k) * 2 + c, 32), :] = own[i * 4 + k]
            w_ref[at((i * 4 + k) * 2 + 1 - c, 32), :] = got[i * 4 + k]
        return nothing

    lax.fori_loop(0, NZ * NX // 4, chip, 0)
    raw = jnp.dot(t_ref[...], w_ref[...], preferred_element_type=F32).astype(BF16)
    kv_ref[:, :HEAD_DIM] = rotated(raw[:, :HEAD_DIM], gain[...], cosine[...], sine[...], 1.0)
    kv_ref[:, HEAD_DIM:] = raw[:, HEAD_DIM:]


def q_kernel(i_ref, t_ref, column, rest, got, gain, cosine, sine, q_ref, w_ref):
    fill_rows(i_ref, w_ref, column, rest, got)
    raw = jnp.dot(t_ref[...], w_ref[...], preferred_element_type=F32).astype(BF16)
    rows = raw.shape[0]
    scale = HEAD_DIM ** (-0.5) * math.log2(math.e)
    for h in range(GROUP):
        head = raw[:, h * HEAD_DIM : (h + 1) * HEAD_DIM]
        q_ref[h * rows : (h + 1) * rows, :] = rotated(head, gain[...], cosine[...], sine[...], scale)


def attend_kernel(*refs, pieces, chunk, first, last, offset):
    q_ref, *kv_refs = refs[: 1 + pieces]
    ins = refs[1 + pieces : 1 + pieces + (0 if first else 2)]
    *outs, k_ref, v_ref = refs[1 + pieces + len(ins) :]
    for i, ref in enumerate(kv_refs):
        keys = slice(i * ref.shape[0], (i + 1) * ref.shape[0])
        k_ref[:, keys] = ref[:, :HEAD_DIM].T
        v_ref[keys, :HEAD_DIM] = ref[:, HEAD_DIM:]
    v_ref[:, HEAD_DIM:] = jnp.ones((v_ref.shape[0], HEAD_DIM), BF16)
    sub = 128
    lane = lax.broadcasted_iota(jnp.int32, (sub, HEAD_DIM), 1)

    def part(t, nothing):
        def rows(r, start=0):
            return pl.ds(pl.multiple_of(t * chunk + r, sub) + start, sub)

        def scores(r):
            return jnp.dot(q_ref[rows(r, offset)], k_ref[...], preferred_element_type=F32)

        following = scores(0)
        for r in range(0, chunk, sub):
            s = following
            if r + sub < chunk:
                following = scores(r + sub)
            best = jnp.max(s, axis=1, keepdims=True)
            if not first:
                old = ins[0][rows(r, offset), :1]
                best = jnp.maximum(best, old)
            weights = jnp.exp2(s - best).astype(BF16)
            acc = jnp.dot(weights, v_ref[...], preferred_element_type=F32)
            if not first:
                acc = acc + ins[1][rows(r, offset)] * jnp.exp2(old - best)
            if last:
                outs[0][rows(r), :HEAD_DIM] = acc[:, :HEAD_DIM]
                outs[0][rows(r), HEAD_DIM:] = jnp.where(lane < 64, acc[:, HEAD_DIM:], best)
            else:
                outs[0][rows(r)] = jnp.broadcast_to(best, (sub, HEAD_DIM))
                outs[1][rows(r)] = acc
        return nothing

    lax.fori_loop(0, outs[0].shape[0] // chunk, part, 0)


def attend(q, kvs, carry, chunk, last=None):
    first, count = carry is None, kvs[0].shape[0]
    rows = q.shape[0] // (1 if last is None else 2)
    shapes = [jax.ShapeDtypeStruct((rows, n), F32) for n in ((HEAD_DIM, 2 * HEAD_DIM) if last is None else (2 * HEAD_DIM,))]
    pieces = len(kvs)
    out = pl.pallas_call(
        functools.partial(attend_kernel, pieces=pieces, chunk=chunk, first=first, last=last is not None, offset=(last or 0) * rows),
        in_specs=[WHOLE] * (1 + pieces + (0 if first else 2)),
        out_specs=[WHOLE] * len(shapes),
        out_shape=shapes,
        scratch_shapes=[
            pltpu.VMEM((HEAD_DIM, pieces * count), BF16),
            pltpu.VMEM((pieces * count, 2 * HEAD_DIM), BF16),
        ],
        input_output_aliases={} if first or last is not None else {1 + pieces: 0, 2 + pieces: 1},
        compiler_params=pltpu.CompilerParams(vmem_limit_bytes=40 * 2**20),
        cost_estimate=pl.CostEstimate(
            flops=8 * rows * count * HEAD_DIM * pieces, bytes_accessed=8 * 2**20, transcendentals=rows * count
        ),
        name="attend",
    )(q, *kvs, *([] if first else carry))
    return out if last is None else out[0]


def project_out_kernel(i_ref, own_ref, got_ref, column, rest, rest_got, out_ref, w_ref, at_ref):
    fill_rows(i_ref, w_ref, column, rest, rest_got)
    rows = own_ref.shape[0] // GROUP
    for h in range(GROUP):
        mine, theirs = own_ref[h * rows : (h + 1) * rows], got_ref[h * rows : (h + 1) * rows]
        best_a, best_b = mine[:, 255:256], theirs[:, 255:256]
        top = jnp.maximum(best_a, best_b)
        both = mine * jnp.exp2(best_a - top) + theirs * jnp.exp2(best_b - top)
        at_ref[:, h * HEAD_DIM : (h + 1) * HEAD_DIM] = (both[:, :HEAD_DIM] / both[:, HEAD_DIM : HEAD_DIM + 1]).astype(BF16)
    out_ref[...] = lax.dot_general(
        at_ref[...], w_ref[...], (((1,), (1,)), ((), ())), preferred_element_type=F32
    ).astype(BF16)


def tables(positions):
    lane = jnp.arange(HEAD_DIM)
    f = lane % 32
    inverse_rate = rope_base ** (-(2 * f).astype(F32) / 64)
    row = (positions // GRID_W).astype(F32)
    column = (positions % GRID_W).astype(F32)
    place = jnp.where(lane[None] < 64, row[:, None], column[:, None])
    angle = place * inverse_rate[None]
    return jnp.cos(angle), jnp.sin(angle) * jnp.where((lane // 32) % 2 == 0, -1.0, 1.0)


def start_x(column, half):
    near = turn(column, X, NX)
    return column, near, shift(half, X, NX, 2)


def finish_x(where, column, near, far):
    (rest,) = call(join_kernel, [((768, near.shape[1]), BF16)], where, near, far)
    return column, rest, other_core(rest)


def local(tokens, query_weight, key_weight, value_weight, out_weight, query_gain, key_gain):
    where = jnp.stack([lax.axis_index(a) for a in (Z, X, C, Y)]).astype(jnp.int32)
    rows = tokens.shape[0] * NY
    positions = lax.axis_index(SP) * rows + jnp.arange(rows, dtype=jnp.int32)
    cosine, sine = tables(positions)
    gain_q, gain_k = query_gain[None], key_gain[None]

    kv_weight = everyone(jnp.concatenate([key_weight, value_weight], axis=1), (Z, X))
    w_own = jnp.concatenate([query_weight, out_weight.T], axis=1)
    w_other = other_core(w_own)
    slab = jnp.concatenate([w_own, w_other], axis=0)
    leaps = leap(slab, 1), leap(slab, 2), leap(slab, 3)
    leaps += (leap(w_own, 4),)
    toks = [tokens] + [shift(tokens, Y, NY, -by) for by in (1, 2, 3)]
    kv_got = other_core(kv_weight)

    kv_own, rows_in = call(
        kv_kernel, [((rows, 256), BF16), ((rows, tokens.shape[1]), BF16)],
        where, *toks, kv_weight, kv_got, gain_k, cosine, sine,
        scratch=[pltpu.VMEM((tokens.shape[1], 256), BF16)],
    )
    mine = jnp.concatenate(after(leaps, kv_own), axis=0)
    got = other_core(mine)
    q_column, q_half, wo_column, wo_half = call(
        column_kernel, [((512, 512), BF16), ((256, 512), BF16)] * 2, where, w_own, w_other, mine, got,
    )
    parts = [shift(kv_own, X, NX, by) for by in (2, 1, 3)]
    plane = jnp.concatenate([kv_own, *parts], axis=0)

    (q_own,) = call(
        q_kernel, [((GROUP * rows, HEAD_DIM), BF16)],
        where, rows_in, *finish_x(where, *start_x(q_column, q_half)), gain_q, cosine, sine,
        scratch=[pltpu.VMEM((tokens.shape[1], 512), BF16)],
    )
    q_all = jnp.concatenate([q_own, other_core(q_own)], axis=0)
    wo_column, *wo_parts = start_x(wo_column, wo_half)

    chain = {"a": plane, "b": other_core(plane)}
    carry, todo = None, [plane]
    for step in range(1, 5):
        for name in "ab" if step < 4 else "a":
            chain[name] = turn(chain[name], Z, NZ)
            todo.append(chain[name])
    for i, at_once in enumerate((todo[0:2], todo[2:3], todo[3:5], todo[5:7])):
        carry = attend(q_all, at_once, carry, 1024 if i in (1, 3) else 512)
        if i == 1:
            wo_all = finish_x(where, wo_column, *wo_parts)
    theirs = attend(q_all, todo[7:], carry, 1024, last=1)
    got = other_core(theirs)
    own = attend(q_all, todo[7:], carry, 1024, last=0)
    (partial,) = call(
        project_out_kernel, [((rows, tokens.shape[1]), BF16)], where, own, got, *wo_all,
        scratch=[pltpu.VMEM((2048, 512), BF16), pltpu.VMEM((rows, GROUP * HEAD_DIM), BF16)],
    )
    pieces = partial.reshape(NY, -1, partial.shape[1])
    summed = jnp.sum(lax.all_to_all(pieces, Y, 0, 0).astype(F32), axis=0)
    mixed = summed * lax.rsqrt(jnp.mean(summed * summed, axis=-1, keepdims=True) + eps)
    return mixed.astype(BF16)


def solution(mesh):
    split = Mesh(mesh.devices.reshape(NZ, NX, NC, NY), SP_TP)

    return jax.shard_map(
        local,
        mesh=split,
        in_specs=(P(SP_TP, None), P(SP, Y), P(SP, Y), P(SP, Y), P(Y, SP), P(), P()),
        out_specs=P(SP_TP, None),
        check_vma=False,
    )
```

```python
import functools
import math

import jax
import jax.numpy as jnp
from jax import lax
from jax.experimental import pallas as pl
from jax.experimental.pallas import tpu as pltpu
from jax.sharding import Mesh
from jax.sharding import PartitionSpec as P


HEAD_DIM = 128
GROUP = 4
GRID_W = 64
Z, X, C, Y = "sp_0", "sp_1", "sp_2", "tp"
SP = (Z, X, C)
SP_TP = (Z, X, C, Y)
NZ, NX, NC, NY = 8, 4, 2, 4

eps = 1e-06
rope_base = 10000.0

F32 = jnp.float32
BF16 = jnp.bfloat16
WHOLE = pl.BlockSpec(memory_space=pltpu.VMEM)
SCALARS = pl.BlockSpec(memory_space=pltpu.SMEM)


def other_core(piece):
    return lax.ppermute(piece, C, [(0, 1), (1, 0)])


def turn(piece, axis, count):
    pairs = []
    for i in range(count):
        pairs += [(i * 2, (i + 1) % count * 2), (i * 2 + 1, (i - 1) % count * 2 + 1)]
    return lax.ppermute(piece, (axis, C), pairs)


def shift(piece, axis, count, by):
    return lax.ppermute(piece, axis, [(i, (i + by) % count) for i in range(count)])


def leap(piece, by):
    pairs = []
    for i in range(NZ):
        pairs += [(i * 2, (i + by) % NZ * 2), (i * 2 + 1, (i - by) % NZ * 2 + 1)]
    return lax.ppermute(piece, (Z, C), pairs)


def everyone(piece, axes):
    n = lax.axis_size(axes)
    return lax.all_to_all(jnp.broadcast_to(piece[None], (n,) + piece.shape), axes, 0, 0)


def after(value, *events):
    return lax.optimization_barrier((value, *events))[0]


def call(kernel, outs, *args, scratch=(), flops=0):
    return pl.pallas_call(
        kernel,
        in_specs=[SCALARS] + [WHOLE] * (len(args) - 1),
        out_specs=[WHOLE] * len(outs),
        out_shape=[jax.ShapeDtypeStruct(s, d) for s, d in outs],
        scratch_shapes=list(scratch),
        compiler_params=pltpu.CompilerParams(vmem_limit_bytes=40 * 2**20),
        cost_estimate=pl.CostEstimate(flops=flops, bytes_accessed=4 * 2**20, transcendentals=0),
    )(*args)


def at(index, size):
    return pl.ds(pl.multiple_of(index * size, size), size)


def column_kernel(i_ref, own_ref, other_ref, mine_ref, got_ref, q_ref, q_half_ref, o_ref, o_half_ref):
    z, c = i_ref[0], i_ref[2]
    away = 1 - 2 * c
    width = q_ref.shape[1]

    def put(ref, start, plane, half):
        place = at(half * NZ + (plane + 2 * NZ) % NZ, 32)
        q_ref[place, :] = ref[start : start + 32, :width]
        o_ref[place, :] = ref[start : start + 32, width:]

    put(own_ref, 0, z, c)
    put(other_ref, 0, z, 1 - c)
    for s in range(1, 4):
        for j in range(2):
            half = jnp.where(c == 0, j, 1 - j)
            start = s * 64 - 64 + j * 32
            put(mine_ref, start, z - away * s, half)
            put(got_ref, start, z + away * s, 1 - half)
    put(mine_ref, 192, z + 4, c)
    put(got_ref, 192, z + 4, 1 - c)
    q_half_ref[...] = q_ref[at(c, 256), :]
    o_half_ref[...] = o_ref[at(c, 256), :]


def join_kernel(i_ref, near_ref, far_ref, out_ref):
    out_ref[:512, :] = near_ref[...]
    out_ref[512:, :] = far_ref[...]


def fill_rows(i_ref, w_ref, column, rest, got):
    x, c = i_ref[1], i_ref[2]
    minus = (x + jnp.where(c == 0, 3, 1)) % NX
    plus = (x + jnp.where(c == 0, 1, 3)) % NX
    opposite = (x + 2) % NX

    def plane(z, nothing):
        row = pl.multiple_of(z * 32, 32)
        for k in range(2):
            place = pl.ds(row + k * 256, 32)
            for ref, where in ((column, x), (rest, minus), (got, plus)):
                w_ref[at((z * NX + where) * 2 + k, 32), :] = ref[place, :]
        w_ref[at((z * NX + opposite) * 2 + c, 32), :] = rest[pl.ds(row + 512, 32), :]
        w_ref[at((z * NX + opposite) * 2 + 1 - c, 32), :] = got[pl.ds(row + 512, 32), :]
        return nothing

    lax.fori_loop(0, NZ, plane, 0)


def rotated(raw, gain, cosine, sine, scale):
    wide = raw.astype(F32)
    n = wide * lax.rsqrt(jnp.mean(wide * wide, axis=-1, keepdims=True) + eps) * gain
    lane = lax.broadcasted_iota(jnp.int32, n.shape, 1)
    swapped = jnp.where(lane // 32 % 2 == 0, pltpu.roll(n, 96, 1), pltpu.roll(n, 32, 1))
    return ((n * cosine + swapped * sine) * scale).astype(BF16)


def kv_kernel(i_ref, t0, t1, t2, t3, own, got, gain, cosine, sine, kv_ref, t_ref, w_ref):
    c, y = i_ref[2], i_ref[3]
    for by, ref in enumerate((t0, t1, t2, t3)):
        t_ref[at((y + by) % NY, 64), :] = ref[...]

    def chip(i, nothing):
        for k in range(4):
            w_ref[at((i * 4 + k) * 2 + c, 32), :] = own[i * 4 + k]
            w_ref[at((i * 4 + k) * 2 + 1 - c, 32), :] = got[i * 4 + k]
        return nothing

    lax.fori_loop(0, NZ * NX // 4, chip, 0)
    raw = jnp.dot(t_ref[...], w_ref[...], preferred_element_type=F32).astype(BF16)
    kv_ref[:, :HEAD_DIM] = rotated(raw[:, :HEAD_DIM], gain[...], cosine[...], sine[...], 1.0)
    kv_ref[:, HEAD_DIM:] = raw[:, HEAD_DIM:]


def q_kernel(i_ref, t_ref, column, rest, got, gain, cosine, sine, q_ref, w_ref):
    fill_rows(i_ref, w_ref, column, rest, got)
    raw = jnp.dot(t_ref[...], w_ref[...], preferred_element_type=F32).astype(BF16)
    rows = raw.shape[0]
    scale = HEAD_DIM ** (-0.5) * math.log2(math.e)
    for h in range(GROUP):
        head = raw[:, h * HEAD_DIM : (h + 1) * HEAD_DIM]
        q_ref[h * rows : (h + 1) * rows, :] = rotated(head, gain[...], cosine[...], sine[...], scale)


def attend_kernel(*refs, pieces, chunk, first, last, offset):
    q_ref, *kv_refs = refs[: 1 + pieces]
    ins = refs[1 + pieces : 1 + pieces + (0 if first else 2)]
    *outs, k_ref, v_ref = refs[1 + pieces + len(ins) :]
    for i, ref in enumerate(kv_refs):
        keys = slice(i * ref.shape[0], (i + 1) * ref.shape[0])
        k_ref[:, keys] = ref[:, :HEAD_DIM].T
        v_ref[keys, :HEAD_DIM] = ref[:, HEAD_DIM:]
    v_ref[:, HEAD_DIM:] = jnp.ones((v_ref.shape[0], HEAD_DIM), BF16)
    sub = 128
    lane = lax.broadcasted_iota(jnp.int32, (sub, HEAD_DIM), 1)

    def part(t, nothing):
        def rows(r, start=0):
            return pl.ds(pl.multiple_of(t * chunk + r, sub) + start, sub)

        def scores(r):
            return jnp.dot(q_ref[rows(r, offset)], k_ref[...], preferred_element_type=F32)

        following = scores(0)
        for r in range(0, chunk, sub):
            s = following
            if r + sub < chunk:
                following = scores(r + sub)
            best = jnp.max(s, axis=1, keepdims=True)
            if not first:
                old = ins[0][rows(r, offset), :1]
                best = jnp.maximum(best, old)
            weights = jnp.exp2(s - best).astype(BF16)
            acc = jnp.dot(weights, v_ref[...], preferred_element_type=F32)
            if not first:
                acc = acc + ins[1][rows(r, offset)] * jnp.exp2(old - best)
            if last:
                outs[0][rows(r), :HEAD_DIM] = acc[:, :HEAD_DIM]
                outs[0][rows(r), HEAD_DIM:] = jnp.where(lane < 64, acc[:, HEAD_DIM:], best)
            else:
                outs[0][rows(r)] = jnp.broadcast_to(best, (sub, HEAD_DIM))
                outs[1][rows(r)] = acc
        return nothing

    lax.fori_loop(0, outs[0].shape[0] // chunk, part, 0)


def attend(q, kvs, carry, chunk, last=None):
    first, count = carry is None, kvs[0].shape[0]
    rows = q.shape[0] // (1 if last is None else 2)
    shapes = [jax.ShapeDtypeStruct((rows, n), F32) for n in ((HEAD_DIM, 2 * HEAD_DIM) if last is None else (2 * HEAD_DIM,))]
    pieces = len(kvs)
    out = pl.pallas_call(
        functools.partial(attend_kernel, pieces=pieces, chunk=chunk, first=first, last=last is not None, offset=(last or 0) * rows),
        in_specs=[WHOLE] * (1 + pieces + (0 if first else 2)),
        out_specs=[WHOLE] * len(shapes),
        out_shape=shapes,
        scratch_shapes=[
            pltpu.VMEM((HEAD_DIM, pieces * count), BF16),
            pltpu.VMEM((pieces * count, 2 * HEAD_DIM), BF16),
        ],
        input_output_aliases={} if first or last is not None else {1 + pieces: 0, 2 + pieces: 1},
        compiler_params=pltpu.CompilerParams(vmem_limit_bytes=40 * 2**20),
        cost_estimate=pl.CostEstimate(
            flops=8 * rows * count * HEAD_DIM * pieces, bytes_accessed=8 * 2**20, transcendentals=rows * count
        ),
        name="attend",
    )(q, *kvs, *([] if first else carry))
    return out if last is None else out[0]


def fill_kernel(i_ref, column, rest, got, w_ref):
    fill_rows(i_ref, w_ref, column, rest, got)


def project_out_kernel(i_ref, own_ref, got_ref, w_ref, out_ref, at_ref):
    rows = own_ref.shape[0] // GROUP
    for h in range(GROUP):
        mine, theirs = own_ref[h * rows : (h + 1) * rows], got_ref[h * rows : (h + 1) * rows]
        best_a, best_b = mine[:, 255:256], theirs[:, 255:256]
        top = jnp.maximum(best_a, best_b)
        both = mine * jnp.exp2(best_a - top) + theirs * jnp.exp2(best_b - top)
        at_ref[:, h * HEAD_DIM : (h + 1) * HEAD_DIM] = (both[:, :HEAD_DIM] / both[:, HEAD_DIM : HEAD_DIM + 1]).astype(BF16)
    out_ref[...] = lax.dot_general(
        at_ref[...], w_ref[...], (((1,), (1,)), ((), ())), preferred_element_type=F32
    ).astype(BF16)


def tables(positions):
    lane = jnp.arange(HEAD_DIM)
    f = lane % 32
    inverse_rate = rope_base ** (-(2 * f).astype(F32) / 64)
    row = (positions // GRID_W).astype(F32)
    column = (positions % GRID_W).astype(F32)
    place = jnp.where(lane[None] < 64, row[:, None], column[:, None])
    angle = place * inverse_rate[None]
    return jnp.cos(angle), jnp.sin(angle) * jnp.where((lane // 32) % 2 == 0, -1.0, 1.0)


def start_x(column, half):
    near = turn(column, X, NX)
    return column, near, shift(half, X, NX, 2)


def finish_x(where, column, near, far):
    (rest,) = call(join_kernel, [((768, near.shape[1]), BF16)], where, near, far)
    return column, rest, other_core(rest)


def local(tokens, query_weight, key_weight, value_weight, out_weight, query_gain, key_gain):
    where = jnp.stack([lax.axis_index(a) for a in (Z, X, C, Y)]).astype(jnp.int32)
    rows = tokens.shape[0] * NY
    positions = lax.axis_index(SP) * rows + jnp.arange(rows, dtype=jnp.int32)
    cosine, sine = tables(positions)
    gain_q, gain_k = query_gain[None], key_gain[None]

    kv_weight = everyone(jnp.concatenate([key_weight, value_weight], axis=1), (Z, X))
    w_own = jnp.concatenate([query_weight, out_weight.T], axis=1)
    w_other = other_core(w_own)
    slab = jnp.concatenate([w_own, w_other], axis=0)
    leaps = leap(slab, 1), leap(slab, 2), leap(slab, 3)
    leaps += (leap(w_own, 4),)
    toks = [tokens] + [shift(tokens, Y, NY, -by) for by in (1, 2, 3)]
    kv_got = other_core(kv_weight)

    kv_own, rows_in = call(
        kv_kernel, [((rows, 256), BF16), ((rows, tokens.shape[1]), BF16)],
        where, *toks, kv_weight, kv_got, gain_k, cosine, sine,
        scratch=[pltpu.VMEM((tokens.shape[1], 256), BF16)],
    )
    mine = jnp.concatenate(after(leaps, kv_own), axis=0)
    got = other_core(mine)
    q_column, q_half, wo_column, wo_half = call(
        column_kernel, [((512, 512), BF16), ((256, 512), BF16)] * 2, where, w_own, w_other, mine, got,
    )
    parts = [shift(kv_own, X, NX, by) for by in (2, 1, 3)]
    plane = jnp.concatenate([kv_own, *parts], axis=0)

    (q_own,) = call(
        q_kernel, [((GROUP * rows, HEAD_DIM), BF16)],
        where, rows_in, *finish_x(where, *start_x(q_column, q_half)), gain_q, cosine, sine,
        scratch=[pltpu.VMEM((tokens.shape[1], 512), BF16)],
    )
    q_all = jnp.concatenate([q_own, other_core(q_own)], axis=0)
    wo_column, *wo_parts = start_x(wo_column, wo_half)

    chain = {"a": plane, "b": other_core(plane)}
    carry, todo = None, [plane]
    for step in range(1, 5):
        for name in "ab" if step < 4 else "a":
            chain[name] = turn(chain[name], Z, NZ)
            todo.append(chain[name])
    for i, at_once in enumerate((todo[0:2], todo[2:3], todo[3:5], todo[5:7])):
        carry = attend(q_all, at_once, carry, 1024 if i in (1, 3) else 512)
        if i == 1:
            wo_all = finish_x(where, wo_column, *wo_parts)
    theirs = attend(q_all, todo[7:], carry, 1024, last=1)
    got = other_core(theirs)
    own = attend(q_all, todo[7:], carry, 1024, last=0)
    (wo_rows,) = call(fill_kernel, [((tokens.shape[1], GROUP * HEAD_DIM), BF16)], where, *wo_all)
    (partial,) = call(
        project_out_kernel, [((rows, tokens.shape[1]), BF16)], where, own, got, wo_rows,
        scratch=[pltpu.VMEM((rows, GROUP * HEAD_DIM), BF16)],
    )
    pieces = partial.reshape(NY, -1, partial.shape[1])
    summed = jnp.sum(lax.all_to_all(pieces, Y, 0, 0).astype(F32), axis=0)
    mixed = summed * lax.rsqrt(jnp.mean(summed * summed, axis=-1, keepdims=True) + eps)
    return mixed.astype(BF16)


def solution(mesh):
    split = Mesh(mesh.devices.reshape(NZ, NX, NC, NY), SP_TP)

    return jax.shard_map(
        local,
        mesh=split,
        in_specs=(P(SP_TP, None), P(SP, Y), P(SP, Y), P(SP, Y), P(Y, SP), P(), P()),
        out_specs=P(SP_TP, None),
        check_vma=False,
    )
```
